512 devices in a mesh: sp: 64 (over z, y), fs: 4 (over x), tp: 2 (over core).
Axes of the slice: x: 4, y: 8, z: 8, core: 2. Of those that a mesh axis runs over, the one named last changes fastest.
Arguments:
- q_latent: bfloat16 [16384, 512], P('sp'), may hold values from -6 to 6
- kv_latent: bfloat16 [16384, 256], P('sp'), may hold values from -6 to 6
- key_rope: bfloat16 [16384, 64], P('sp'), may hold values from -6 to 6
- pool_input: bfloat16 [16384, 1024], P('sp', 'fs'), may hold values from -6 to 6
- q_lat_gain: float32 [512], replicated, may hold values from 0.1 to 1.9
- kv_lat_gain: float32 [256], replicated, may hold values from 0.1 to 1.9
- q_head_gain: float32 [192], replicated, may hold values from 1 to 4.2
- k_head_gain: float32 [192], replicated, may hold values from 1 to 4.2
- pool_gain: float32 [1024], P(('fs', 'tp')), may hold values from 0.1 to 1.9
- q_up: bfloat16 [512, 3072], P(None, ('fs', 'tp')), may hold values from -1 to 1
- key_up: bfloat16 [256, 2048], P(None, ('fs', 'tp')), may hold values from -1 to 1
- value_up: bfloat16 [256, 2048], P(None, ('fs', 'tp')), may hold values from -0.375 to 0.375
- pool_mix: bfloat16 [4, 256, 256], P('fs', None, 'tp'), may hold values from -0.375 to 0.375
- out_pool: bfloat16 [1024, 4096], P(('fs', 'tp')), may hold values from -0.109375 to 0.109375
- out_attn: bfloat16 [2048, 4096], P(('fs', 'tp')), may hold values from -0.109375 to 0.109375
Outputs:
- mixed: bfloat16 [16384, 4096], P(('sp', 'fs', 'tp'))
- log_weight: float32 [16, 16384], P(('fs', 'tp'), 'sp')
The draws below stay inside these ranges and needn't reach their ends.
All inputs are finite; a program needn't handle non-finite values.
Results may differ from the reference program's by a relative error of at most 0.015.
Values may be sent and summed in bfloat16 or wider, within the bound.
No kernel may reach another device: no remote copies, remote signals or barrier semaphores. Data moves between devices by JAX's collectives and lax.ppermute only.
A program may use at most 128 MiB of HBM per device.

```python
import math
import jax
import jax.numpy as jnp
from jax import lax

D = 4096
H = 16
NOPE = 128
ROPE = 64
VD = 128
RQ = 512
KVR = 256
P_SIZE = 1024
SCALES = 4
G = 256
L = 16384
N_FS = 4
N_TP = 2


def plant_plan(key):
    base_key = jax.random.fold_in(key, 7001)
    split_keys = jax.random.split(base_key, 5)
    channels = jax.random.randint(split_keys[0], (H,), 0, NOPE)
    query_dirs = jnp.clip(jax.random.normal(split_keys[1], (H, RQ), jnp.float32), -6.0, 6.0)
    key_dirs = jnp.clip(jax.random.normal(split_keys[2], (H, KVR), jnp.float32), -6.0, 6.0)
    half_length = L // 2
    key_rows = jax.random.permutation(split_keys[3], half_length)[:2 * H]
    query_rows = half_length + jax.random.permutation(split_keys[4], L - half_length)[:2 * H]
    owners = jnp.arange(2 * H, dtype=jnp.int32) % H
    return (channels, query_dirs, key_dirs, key_rows, query_rows, owners)


def unit_rows(directions):
    return directions / jnp.sqrt(jnp.sum(directions * directions, axis=1, keepdims=True))


def draw_q_latent(key, part):
    channels, query_dirs, key_dirs, key_rows, query_rows, owners = plant_plan(key)
    own_key = jax.random.fold_in(key, 7101)
    drawn = jnp.clip(jax.random.normal(own_key, (L, RQ), jnp.float32), -6.0, 6.0)
    return drawn.at[query_rows].set(query_dirs[owners]).astype(jnp.bfloat16)


def draw_kv_latent(key, part):
    channels, query_dirs, key_dirs, key_rows, query_rows, owners = plant_plan(key)
    own_key = jax.random.fold_in(key, 7102)
    drawn = jnp.clip(jax.random.normal(own_key, (L, KVR), jnp.float32), -6.0, 6.0)
    return drawn.at[key_rows].set(key_dirs[owners]).astype(jnp.bfloat16)


def draw_q_up(key, part):
    channels, query_dirs, key_dirs, key_rows, query_rows, owners = plant_plan(key)
    own_key = jax.random.fold_in(key, 7103)
    drawn = jnp.clip(jax.random.normal(own_key, (RQ, H * (NOPE + ROPE)), jnp.float32), -6.0, 6.0) * RQ ** (-0.5)
    columns = jnp.arange(H, dtype=jnp.int32) * (NOPE + ROPE) + channels
    planted = drawn.at[:, columns].set(jnp.transpose(unit_rows(query_dirs)))
    return jnp.clip(planted, -1.0, 1.0).astype(jnp.bfloat16)


def draw_key_up(key, part):
    channels, query_dirs, key_dirs, key_rows, query_rows, owners = plant_plan(key)
    own_key = jax.random.fold_in(key, 7104)
    drawn = jnp.clip(jax.random.normal(own_key, (KVR, H * NOPE), jnp.float32), -6.0, 6.0) * KVR ** (-0.5)
    columns = jnp.arange(H, dtype=jnp.int32) * NOPE + channels
    planted = drawn.at[:, columns].set(jnp.transpose(unit_rows(key_dirs)))
    return jnp.clip(planted, -1.0, 1.0).astype(jnp.bfloat16)


def planted_gain(key, salt):
    channels, query_dirs, key_dirs, key_rows, query_rows, owners = plant_plan(key)
    own_key = jax.random.fold_in(key, salt)
    split_keys = jax.random.split(own_key, 2)
    drawn = jnp.exp(jax.random.uniform(split_keys[0], (NOPE + ROPE,), jnp.float32, 0.0, 1.0986123))
    strong = jax.random.uniform(split_keys[1], (H,), jnp.float32, 3.6, 4.2)
    return drawn.at[channels].set(strong)


def draw_q_head_gain(key, part):
    return planted_gain(key, 7105)


def draw_k_head_gain(key, part):
    return planted_gain(key, 7106)


def level_of(key, extent, shards, smallest, high):
    def one(dim, parts):
        heights = jax.random.uniform(jax.random.fold_in(jax.random.fold_in(key, 6), dim), (parts,), jnp.float32, smallest / len(shards), high / len(shards))
        return jnp.repeat(jnp.exp(heights), extent[dim] // parts).reshape((-1,) + (1,) * (len(extent) - dim - 1))

    gain = one(*shards[0])
    for cut in shards[1:]:
        gain = gain * one(*cut)
    return gain


def centred(stream_key, extent, spread, bound, cuts=(), kind=jnp.bfloat16):
    drawn = jax.random.normal(stream_key, extent, jnp.float32) * spread
    if len(cuts) > 0:
        drawn = level_of(stream_key, extent, cuts, -0.22, 0.18) * drawn
    return jnp.clip(drawn, min=-bound, max=bound).astype(kind)


def setup_inputs(seed: int = 0) -> dict:
    seeds = jax.random.split(jax.random.key(seed), 16)
    return {
        "q_latent": draw_q_latent(jax.random.fold_in(seeds[15], 71), 0),
        "kv_latent": draw_kv_latent(jax.random.fold_in(seeds[15], 71), 0),
        "key_rope": centred(seeds[2], (L, ROPE), 1.0, 6.0, ((0, 64),)),
        "pool_input": centred(seeds[3], (L, P_SIZE), 1.0, 6.0, ((0, 64), (1, 4))),
        "q_lat_gain": jnp.clip(1.0 + 0.18 * jax.random.normal(seeds[4], (RQ,), jnp.float32), 0.1, 1.9),
        "kv_lat_gain": jnp.clip(1.0 + 0.18 * jax.random.normal(seeds[5], (KVR,), jnp.float32), 0.1, 1.9),
        "q_head_gain": draw_q_head_gain(jax.random.fold_in(seeds[15], 71), 0),
        "k_head_gain": draw_k_head_gain(jax.random.fold_in(seeds[15], 71), 0),
        "pool_gain": jnp.clip(1.0 + 0.18 * jax.random.normal(seeds[8], (P_SIZE,), jnp.float32), 0.1, 1.9),
        "q_up": draw_q_up(jax.random.fold_in(seeds[15], 71), 0),
        "key_up": draw_key_up(jax.random.fold_in(seeds[15], 71), 0),
        "value_up": centred(seeds[11], (KVR, H * VD), KVR ** -0.5, 0.375, ((1, 8),)),
        "pool_mix": centred(seeds[12], (SCALES, G, G), G ** -0.5, 0.375, ((0, 4), (2, 2))),
        "out_pool": centred(seeds[13], (P_SIZE, D), (P_SIZE + H * VD) ** -0.5, 0.109375, ((0, 8),)),
        "out_attn": centred(seeds[14], (H * VD, D), (P_SIZE + H * VD) ** -0.5, 0.109375, ((0, 8),)),
    }


EPS = 1e-06
THETA = 10000.0

def row_norm(values, row_gain):
    mean_sq = lax.optimization_barrier(jnp.mean(values * values, axis=-1, keepdims=True))
    return values * lax.rsqrt(mean_sq + EPS) * row_gain

def rotate(values, position):
    half_width = values.shape[-1] // 2
    frequency = 1.0 / THETA ** (jnp.arange(0, 2 * half_width, 2, dtype=jnp.float32) / (2 * half_width))
    angles = position.astype(jnp.float32)[:, None] * frequency[None, :]
    cosine_table = jnp.cos(angles)[:, None, :]
    sine_table = jnp.sin(angles)[:, None, :]
    first_half = values[..., :half_width]
    second_half = values[..., half_width:]
    return jnp.concatenate([first_half * cosine_table - second_half * sine_table, first_half * sine_table + second_half * cosine_table], axis=-1)

def make_queries(latent, lat_gain, q_up, norm_gain, position):
    row_count = latent.shape[0]
    normed = row_norm(latent.astype(jnp.float32), lat_gain).astype(jnp.bfloat16)
    query = jnp.dot(normed, q_up, preferred_element_type=jnp.float32).reshape(row_count, -1, NOPE + ROPE)
    query = row_norm(query, norm_gain)
    query = jnp.concatenate([query[..., :NOPE], rotate(query[..., NOPE:], position)], axis=-1)
    return (query * (NOPE + ROPE) ** (-0.5)).astype(jnp.bfloat16)

def make_keys(latent, rope_part, key_up, value_up, norm_gain, position):
    row_count = latent.shape[0]
    unrotated = jnp.dot(latent, key_up, preferred_element_type=jnp.float32).reshape(row_count, -1, NOPE)
    head_count = unrotated.shape[1]
    shared = jnp.broadcast_to(rope_part.astype(jnp.float32)[:, None, :], (row_count, head_count, ROPE))
    key_heads = row_norm(jnp.concatenate([unrotated, shared], axis=-1), norm_gain)
    key_heads = jnp.concatenate([key_heads[..., :NOPE], rotate(key_heads[..., NOPE:], position)], axis=-1)
    value_heads = jnp.dot(latent, value_up, preferred_element_type=jnp.float32).reshape(row_count, head_count, VD)
    return (key_heads.astype(jnp.bfloat16), value_heads.astype(jnp.bfloat16))

def reference(q_latent, kv_latent, key_rope, pool_input, q_lat_gain, kv_lat_gain, q_head_gain, k_head_gain, pool_gain, q_up, key_up, value_up, pool_mix, out_pool, out_attn):
    length = q_latent.shape[0]
    position = jnp.arange(length, dtype=jnp.int32)
    queries = make_queries(q_latent, q_lat_gain, q_up, q_head_gain, position)
    kv_normed = row_norm(kv_latent.astype(jnp.float32), kv_lat_gain).astype(jnp.bfloat16)
    key_heads, value_heads = make_keys(kv_normed, key_rope, key_up, value_up, k_head_gain, position)
    keys_wide = key_heads.astype(jnp.float32)
    values_wide = value_heads.astype(jnp.float32)
    block_rows = math.gcd(length, 256)
    block_count = length // block_rows

    def attend_block(arguments):
        query_block, query_pos = arguments
        scores = jnp.einsum('qhd,khd->qhk', query_block.astype(jnp.float32), keys_wide)
        allowed = position[None, None, :] <= query_pos[:, None, None]
        scores = jnp.where(allowed, scores, -jnp.inf)
        row_max = lax.optimization_barrier(jnp.max(scores, axis=-1))
        weights = jnp.exp(scores - row_max[..., None])
        row_sum = lax.optimization_barrier(jnp.sum(weights, axis=-1))
        rounded = weights.astype(jnp.bfloat16).astype(jnp.float32)
        attended = jnp.einsum('qhk,khd->qhd', rounded, values_wide) / row_sum[..., None]
        return (attended.astype(jnp.bfloat16), row_max + jnp.log(row_sum))
    blocks = (queries.reshape(block_count, block_rows, H, NOPE + ROPE), position.reshape(block_count, block_rows))
    attended, log_parts = lax.map(attend_block, blocks)
    attended = attended.reshape(length, H * VD)
    log_weight = jnp.transpose(log_parts.reshape(length, H))
    group_width = P_SIZE // SCALES
    padded = jnp.pad(pool_input.astype(jnp.float32), ((15, 0), (0, 0)))
    pieces = []
    for group in range(SCALES):
        window = 2 ** (group + 1)
        columns = padded[:, group * group_width:(group + 1) * group_width]
        window_sum = jnp.zeros((length, group_width), jnp.float32)
        for lag_rows in range(16):
            if lag_rows < window:
                window_sum = window_sum + columns[15 - lag_rows:15 - lag_rows + length]
        counts = jnp.minimum(position + 1, window).astype(jnp.float32)[:, None]
        pool_diff = (window_sum / counts - columns[15:]).astype(jnp.bfloat16)
        pieces.append(jnp.dot(pool_diff, pool_mix[group], preferred_element_type=jnp.float32))
    pooled = (jnp.concatenate(pieces, axis=-1) * pool_gain).astype(jnp.bfloat16)
    group_count = N_FS * N_TP
    pool_share = P_SIZE // group_count
    attn_share = H * VD // group_count
    total = jnp.zeros((length, out_pool.shape[1]), jnp.float32)
    for member in range(group_count):
        partial_value = jnp.dot(pooled[:, member * pool_share:(member + 1) * pool_share], out_pool[member * pool_share:(member + 1) * pool_share], preferred_element_type=jnp.float32)
        partial_value = partial_value + jnp.dot(attended[:, member * attn_share:(member + 1) * attn_share], out_attn[member * attn_share:(member + 1) * attn_share], preferred_element_type=jnp.float32)
        rounded_part = lax.optimization_barrier(partial_value.astype(jnp.bfloat16))
        total = total + rounded_part.astype(jnp.float32)
    return (total.astype(jnp.bfloat16), log_weight)
```

```python
from functools import partial
import math

import jax
import jax.numpy as jnp
from jax import lax
from jax.experimental import pallas as pl
from jax.experimental.pallas import tpu as pltpu
from jax.sharding import PartitionSpec as P

NOPE = 128
ROPE = 64
VD = 128
EPS = 1e-06
THETA = 10000.0
HUGE = 1e30
LOG2E = math.log2(math.e)
LN2 = math.log(2.0)
HALF = 128
NB = 8


def row_norm(values, row_gain):
    mean_sq = jnp.mean(values * values, axis=-1, keepdims=True)
    return values * lax.rsqrt(mean_sq + EPS) * row_gain


def angle_tables(position):
    frequency = 1.0 / THETA ** (jnp.arange(0, ROPE, 2, dtype=jnp.float32) / ROPE)
    angles = position.astype(jnp.float32)[:, None] * frequency[None, :]
    return jnp.cos(angles), jnp.sin(angles)


def rotate(values, position):
    half_width = values.shape[-1] // 2
    cosine_table, sine_table = angle_tables(position)
    cosine_table = cosine_table[:, None, :]
    sine_table = sine_table[:, None, :]
    first_half = values[..., :half_width]
    second_half = values[..., half_width:]
    return jnp.concatenate(
        [
            first_half * cosine_table - second_half * sine_table,
            first_half * sine_table + second_half * cosine_table,
        ],
        axis=-1,
    )


def make_queries(latent, lat_gain, q_up, norm_gain, key_gain, position):
    row_count = latent.shape[0]
    normed = row_norm(latent.astype(jnp.float32), lat_gain).astype(jnp.bfloat16)
    query = jnp.dot(normed, q_up, preferred_element_type=jnp.float32).reshape(
        row_count, -1, NOPE + ROPE
    )
    query = row_norm(query, norm_gain)
    scale = LOG2E * (NOPE + ROPE) ** (-0.5)
    query = jnp.concatenate(
        [
            query[..., :NOPE] * (key_gain[:NOPE] * scale),
            rotate(query[..., NOPE:], position) * scale,
            jnp.zeros((*query.shape[:2], 256 - NOPE - ROPE), jnp.float32),
        ],
        axis=-1,
    )
    return jnp.transpose(query.astype(jnp.bfloat16), (1, 0, 2))


def attend_kernel(
    first,
    final,
    where_ref,
    keys_ref,
    q_ref,
    key_up_ref,
    value_up_ref,
    gain_ref,
    block_cos_ref,
    block_sin_ref,
    in_cos_ref,
    in_sin_ref,
    *refs,
):
    if first:
        state_in, refs = None, refs
    else:
        state_in, refs = refs[:3], refs[3:]
    if final:
        out_ref, log_ref, max_ref, sum_ref, acc_ref, key_ref = refs
    else:
        max_ref, sum_ref, acc_ref, key_ref = refs
    heads, rows, _ = q_ref.shape
    step = pl.program_id(0)
    own_block, half_offset = where_ref[0], where_ref[1]
    diagonal = own_block // NB
    width = NB * HALF

    @pl.when(step == 0)
    def _():
        if first:
            max_ref[...] = jnp.full(max_ref.shape, -HUGE, jnp.float32)
            sum_ref[...] = jnp.zeros_like(sum_ref)
            acc_ref[...] = jnp.zeros_like(acc_ref)
        else:
            max_ref[...] = state_in[0][...]
            sum_ref[...] = state_in[1][...]
            acc_ref[...] = state_in[2][...]
        key_ref[:, NOPE + ROPE :, :] = jnp.zeros(
            (heads, 256 - NOPE - ROPE, width), key_ref.dtype
        )

    def build_keys():
        for n in range(NB):
            at = pl.ds(n * HALF, HALF)
            raw = jnp.dot(
                key_up_ref[...], keys_ref[n, :256, :], preferred_element_type=jnp.float32
            )
            rope = keys_ref[n, 256:, :].astype(jnp.float32)
            rope_sq = jnp.sum(rope * rope, axis=0, keepdims=True)
            rope = rope * gain_ref[...]
            block_cos, block_sin = block_cos_ref[n], block_sin_ref[n]
            in_cos, in_sin = in_cos_ref[...], in_sin_ref[...]
            cosine = block_cos * in_cos - block_sin * in_sin
            sine = block_sin * in_cos + block_cos * in_sin
            a, b = rope[: ROPE // 2], rope[ROPE // 2 :]
            turned = jnp.concatenate([a * cosine - b * sine, a * sine + b * cosine], axis=0)
            for h in range(heads):
                part = raw[h * NOPE : (h + 1) * NOPE]
                square = jnp.sum(part * part, axis=0, keepdims=True) + rope_sq
                inverse = lax.rsqrt(square * (1.0 / (NOPE + ROPE)) + EPS)
                key_ref[h, :NOPE, at] = (part * inverse).astype(key_ref.dtype)
                key_ref[h, NOPE : NOPE + ROPE, at] = (turned * inverse).astype(key_ref.dtype)

    def attend(masked):
        build_keys()
        latent = jnp.concatenate([keys_ref[n, :256, :] for n in range(NB)], axis=1)
        for h in range(heads):
            scores = jnp.dot(q_ref[h], key_ref[h], preferred_element_type=jnp.float32)
            if masked:
                column = lax.broadcasted_iota(jnp.int32, (rows, width), 1)
                row = lax.broadcasted_iota(jnp.int32, (rows, width), 0)
                key_pos = (
                    (step * NB + column // HALF) * rows + half_offset + column % HALF
                )
                scores = jnp.where(key_pos <= own_block * rows + row, scores, -HUGE)
            before = max_ref[h]
            after = jnp.maximum(before, jnp.max(scores, axis=1, keepdims=True))
            factor = jnp.exp2(before - after)
            weights = jnp.exp2(scores - after[:, :1])
            partial_sum = weights[:, :128]
            for n in range(1, width // 128):
                partial_sum = partial_sum + weights[:, n * 128 : (n + 1) * 128]
            max_ref[h] = after
            sum_ref[h] = sum_ref[h] * factor + partial_sum
            update = lax.dot_general(
                weights.astype(jnp.bfloat16),
                latent,
                (((1,), (1,)), ((), ())),
                preferred_element_type=jnp.float32,
            )
            acc_ref[h] = acc_ref[h] * factor[:, :1] + update

    pl.when(step < diagonal)(lambda: attend(False))
    pl.when(step == diagonal)(lambda: attend(True))

    if final:

        @pl.when(step == pl.num_programs(0) - 1)
        def _():
            for h in range(heads):
                total = jnp.sum(sum_ref[h], axis=1, keepdims=True)
                mean = acc_ref[h] / total
                high = mean.astype(jnp.bfloat16)
                low = (mean - high.astype(jnp.float32)).astype(jnp.bfloat16)
                value = value_up_ref[:, h * VD : (h + 1) * VD]
                out_ref[:, h * VD : (h + 1) * VD] = (
                    jnp.dot(high, value, preferred_element_type=jnp.float32)
                    + jnp.dot(low, value, preferred_element_type=jnp.float32)
                ).astype(out_ref.dtype)
                log_ref[h] = (max_ref[h] + jnp.log2(total)) * LN2


def attend_part(
    keys, own_block, half_offset, queries, key_up, value_up, gain, block_tables, in_tables, state, final
):
    block_count = keys.shape[0]
    heads, rows, _ = queries.shape
    first = state is None
    place = jnp.stack([own_block, half_offset]).astype(jnp.int32)

    def whole(*shape):
        return pl.BlockSpec(shape, lambda i, w: (0,) * len(shape))

    def tile(*shape):
        return pl.BlockSpec(
            shape, lambda i, w: (jnp.minimum(i, w[0] // NB),) + (0,) * (len(shape) - 1)
        )

    state_shapes = [(heads, rows, 128), (heads, rows, 128), (heads, rows, 256)]
    in_specs = [
        tile(NB, 320, HALF),
        whole(heads, rows, 256),
        whole(*key_up.shape),
        whole(*value_up.shape),
        whole(ROPE, 1),
        tile(NB, ROPE // 2, 1),
        tile(NB, ROPE // 2, 1),
        whole(ROPE // 2, HALF),
        whole(ROPE // 2, HALF),
    ]
    operands = [keys, queries, key_up, value_up, gain, *block_tables, *in_tables]
    if not first:
        in_specs += [whole(*s) for s in state_shapes]
        operands += list(state)
    key_scratch = pltpu.VMEM((heads, 256, NB * HALF), jnp.bfloat16)
    if final:
        out_shape = [
            jax.ShapeDtypeStruct((rows, heads * VD), jnp.bfloat16),
            jax.ShapeDtypeStruct((heads, rows, 128), jnp.float32),
        ]
        out_specs = [whole(rows, heads * VD), whole(heads, rows, 128)]
        scratch = [pltpu.VMEM(s, jnp.float32) for s in state_shapes] + [key_scratch]
    else:
        out_shape = [jax.ShapeDtypeStruct(s, jnp.float32) for s in state_shapes]
        out_specs = [whole(*s) for s in state_shapes]
        scratch = [key_scratch]
    flops = 2 * block_count * HALF * heads * rows * 512
    return pl.pallas_call(
        partial(attend_kernel, first, final),
        out_shape=out_shape,
        grid_spec=pltpu.PrefetchScalarGridSpec(
            num_scalar_prefetch=1,
            grid=(block_count // NB,),
            in_specs=in_specs,
            out_specs=out_specs,
            scratch_shapes=scratch,
        ),
        compiler_params=pltpu.CompilerParams(
            dimension_semantics=("arbitrary",), vmem_limit_bytes=60 * 2**20
        ),
        cost_estimate=pl.CostEstimate(
            flops=flops,
            bytes_accessed=keys.size * 2,
            transcendentals=block_count * HALF * heads * rows,
        ),
        name="attend_last" if final else "attend_first",
    )(place, *operands)


def local(
    q_latent,
    kv_latent,
    key_rope,
    pool_input,
    q_lat_gain,
    kv_lat_gain,
    q_head_gain,
    k_head_gain,
    pool_gain,
    q_up,
    key_up,
    value_up,
    pool_mix,
    out_pool,
    out_attn,
):
    row_count = q_latent.shape[0]
    sp_index = lax.axis_index("sp")
    sp_size = lax.axis_size("sp")
    core = lax.axis_index("tp")
    own_pos = sp_index * row_count + jnp.arange(row_count, dtype=jnp.int32)

    share = lax.dynamic_slice_in_dim(kv_latent, core * HALF, HALF, 0)
    share_rope = lax.dynamic_slice_in_dim(key_rope, core * HALF, HALF, 0)
    share = row_norm(share.astype(jnp.float32), kv_lat_gain).astype(jnp.bfloat16)
    share = jnp.concatenate([share.T, share_rope.T], axis=0)
    mine = lax.all_gather(share, "sp", axis=0)
    other = lax.ppermute(mine, "tp", [(0, 1), (1, 0)])

    queries = make_queries(q_latent, q_lat_gain, q_up, q_head_gain, k_head_gain, own_pos)
    head_count = queries.shape[0]
    gain = k_head_gain[NOPE:, None]
    block_tables = [
        t[:, :, None] for t in angle_tables(jnp.arange(sp_size, dtype=jnp.int32) * row_count)
    ]
    offset = core * HALF
    near = [
        t.T for t in angle_tables(offset + jnp.arange(HALF, dtype=jnp.int32))
    ]
    far = [
        t.T for t in angle_tables(HALF - offset + jnp.arange(HALF, dtype=jnp.int32))
    ]
    common = (queries, key_up.T, value_up, gain, block_tables)
    state = attend_part(mine, sp_index, offset, *common, near, None, False)
    attended, log_wide = attend_part(other, sp_index, HALF - offset, *common, far, state, True)
    log_weight = log_wide[:, :, 0]

    earlier = lax.ppermute(
        pool_input[row_count - 15 :], "sp", [(i, i + 1) for i in range(sp_size - 1)]
    )
    extended = jnp.concatenate([earlier, pool_input], axis=0).astype(jnp.float32)
    window = jnp.left_shift(jnp.int32(2), lax.axis_index("fs"))
    window_sum = jnp.zeros((row_count, pool_input.shape[1]), jnp.float32)
    for lag_rows in range(16):
        window_sum = window_sum + jnp.where(
            lag_rows < window, extended[15 - lag_rows : 15 - lag_rows + row_count], 0.0
        )
    counts = jnp.minimum(own_pos + 1, window).astype(jnp.float32)[:, None]
    pool_diff = (window_sum / counts - extended[15:]).astype(jnp.bfloat16)
    pooled = (
        jnp.dot(pool_diff, pool_mix[0], preferred_element_type=jnp.float32) * pool_gain
    ).astype(jnp.bfloat16)
    mixed = lax.psum_scatter(
        (
            jnp.dot(pooled, out_pool, preferred_element_type=jnp.float32)
            + jnp.dot(attended, out_attn, preferred_element_type=jnp.float32)
        ).astype(jnp.bfloat16),
        ("fs", "tp"),
        scatter_dimension=0,
        tiled=True,
    )
    return (mixed, log_weight)


def solution(mesh):
    in_specs = (
        P("sp", None),
        P("sp", None),
        P("sp", None),
        P("sp", "fs"),
        P(),
        P(),
        P(),
        P(),
        P(("fs", "tp")),
        P(None, ("fs", "tp")),
        P(None, ("fs", "tp")),
        P(None, ("fs", "tp")),
        P("fs", None, "tp"),
        P(("fs", "tp"), None),
        P(("fs", "tp"), None),
    )
    out_specs = (P(("sp", "fs", "tp"), None), P(("fs", "tp"), "sp"))
    return jax.shard_map(local, mesh=mesh, in_specs=in_specs, out_specs=out_specs, check_vma=False)
```

```python
import math

import jax
import jax.numpy as jnp
import numpy as np
from jax import lax
from jax.experimental import pallas as pl
from jax.experimental.pallas import tpu as pltpu
from jax.sharding import PartitionSpec as P

NOPE = 128
ROPE = 64
VD = 128
EPS = 1e-06
THETA = 10000.0
HUGE = 1e30
LOG2E = math.log2(math.e)
LN2 = math.log(2.0)
HALF = 128
Y = 8
PLANES = 8
MEMBERS = 4
EXTRA = 16


def turn_tables(block_rows, blocks):
    frequency = 1.0 / THETA ** (np.arange(0, ROPE, 2, dtype=np.float64) / ROPE)
    at_block = (np.arange(blocks) * block_rows)[:, None] * frequency
    within = np.arange(block_rows)[:, None] * frequency
    return [t.astype(np.float32) for a in (at_block, within) for t in (np.cos(a), np.sin(a))]


def row_norm(values, row_gain):
    mean_sq = jnp.mean(values * values, axis=-1, keepdims=True)
    return values * lax.rsqrt(mean_sq + EPS) * row_gain


def make_queries(latent, lat_gain, q_up, norm_gain, key_gain, cosine, sine):
    row_count = latent.shape[0]
    normed = row_norm(latent.astype(jnp.float32), lat_gain).astype(jnp.bfloat16)
    query = jnp.dot(normed, q_up, preferred_element_type=jnp.float32).reshape(
        row_count, -1, NOPE + ROPE
    )
    query = row_norm(query, norm_gain)
    scale = LOG2E * (NOPE + ROPE) ** (-0.5)
    cosine, sine = cosine[:, None, :] * scale, sine[:, None, :] * scale
    a, b = query[..., NOPE : NOPE + ROPE // 2], query[..., NOPE + ROPE // 2 :]
    turned = jnp.concatenate([a * cosine - b * sine, a * sine + b * cosine], axis=-1)
    return jnp.concatenate(
        [
            (query[..., :NOPE] * (key_gain[:NOPE] * scale)).reshape(row_count, -1),
            turned.reshape(row_count, -1),
        ],
        axis=-1,
    ).astype(jnp.bfloat16)


def attend_kernel(
    place_ref,
    mine_ref,
    other_ref,
    q_ref,
    key_up_ref,
    value_up_ref,
    gain_ref,
    block_cos_ref,
    block_sin_ref,
    near_ref,
    far_ref,
    out_ref,
    max_ref,
    sum_ref,
    acc_ref,
    key_ref,
    lat_ref,
):
    heads = key_up_ref.shape[0] // NOPE
    count, rows, _ = q_ref.shape
    step = pl.program_id(0)
    plane, parity, own_y, offset = place_ref[step], place_ref[2], place_ref[3], place_ref[4]
    width = Y * rows

    @pl.when(step == 0)
    def _():
        max_ref[...] = jnp.full(max_ref.shape, -HUGE, jnp.float32)
        sum_ref[...] = jnp.zeros_like(sum_ref)
        acc_ref[...] = jnp.zeros_like(acc_ref)
        key_ref[:, NOPE:, :] = jnp.zeros((heads, 256 - NOPE, width), key_ref.dtype)

    def build_keys():
        @pl.loop(0, Y)
        def _(n):
            for u, (keys_ref, in_ref) in enumerate(((mine_ref, near_ref), (other_ref, far_ref))):
                in_cos, in_sin = in_ref[0], in_ref[1]
                at = pl.ds(pl.multiple_of((u * Y + n) * HALF, HALF), HALF)
                parts = [keys_ref[x, n] for x in range(4)]
                latent = jnp.concatenate([*parts[:3], parts[3][:16]], axis=0)
                lat_ref[:, at] = latent
                raw = jnp.dot(key_up_ref[...], latent, preferred_element_type=jnp.float32)
                rope = parts[3][16:].astype(jnp.float32)
                rope_sq = jnp.sum(rope * rope, axis=0, keepdims=True)
                rope = rope * gain_ref[...]
                block_cos, block_sin = block_cos_ref[n], block_sin_ref[n]
                cosine = block_cos * in_cos - block_sin * in_sin
                sine = block_sin * in_cos + block_cos * in_sin
                a, b = rope[: ROPE // 2], rope[ROPE // 2 :]
                turned = jnp.concatenate([a * cosine - b * sine, a * sine + b * cosine], axis=0)
                for h in range(heads):
                    part = raw[h * NOPE : (h + 1) * NOPE]
                    square = jnp.sum(part * part, axis=0, keepdims=True) + rope_sq
                    inverse = lax.rsqrt(square * (1.0 / (NOPE + ROPE)) + EPS)
                    key_ref[h, :NOPE, at] = (part * inverse).astype(key_ref.dtype)
                    key_ref[h, NOPE + h * ROPE : NOPE + (h + 1) * ROPE, at] = (
                        turned * inverse
                    ).astype(key_ref.dtype)

    def attend(i, h, masked):
        query = jnp.concatenate(
            [q_ref[i, :, pl.ds(pl.multiple_of(h * NOPE, NOPE), NOPE)], q_ref[i, :, heads * NOPE :]], axis=1
        )
        scores = jnp.dot(query, key_ref[h], preferred_element_type=jnp.float32)
        if masked:
            column = lax.broadcasted_iota(jnp.int32, (rows, width), 1)
            row = lax.broadcasted_iota(jnp.int32, (rows, width), 0)
            half_at = jnp.where(column < Y * HALF, offset, HALF - offset)
            key_at = (column % (Y * HALF)) // HALF * rows + half_at + column % HALF
            scores = jnp.where(key_at <= own_y * rows + row, scores, -HUGE)
        at = i * heads + h
        before = max_ref[at]
        after = jnp.maximum(before, jnp.max(scores, axis=1, keepdims=True))
        factor = jnp.exp2(before - after)
        weights = jnp.exp2(scores - after[:, :1])
        partial_sum = weights[:, :128]
        for n in range(1, width // 128):
            partial_sum = partial_sum + weights[:, n * 128 : (n + 1) * 128]
        max_ref[at] = after
        sum_ref[at] = sum_ref[at] * factor + partial_sum
        update = lax.dot_general(
            weights.astype(jnp.bfloat16),
            lat_ref[...],
            (((1,), (1,)), ((), ())),
            preferred_element_type=jnp.float32,
        )
        acc_ref[at] = acc_ref[at] * factor[:, :1] + update

    @pl.when(plane <= parity + 2 * (count - 1))
    def _():
        build_keys()

        @pl.loop(0, count * heads)
        def _(at):
            i, h = at // heads, at % heads
            query_plane = parity + 2 * i
            pl.when(plane < query_plane)(lambda: attend(i, h, False))
            pl.when(plane == query_plane)(lambda: attend(i, h, True))

    @pl.when(step == pl.num_programs(0) - 1)
    def _():
        @pl.loop(0, count)
        def _(i):
            out_ref[i, rows:, :] = jnp.zeros((EXTRA, heads * VD), out_ref.dtype)
            for h in range(heads):
                at = i * heads + h
                total = jnp.sum(sum_ref[at], axis=1, keepdims=True)
                seen = total > 0.0
                total = jnp.where(seen, total, 1.0)
                mean = acc_ref[at] / total
                high = mean.astype(jnp.bfloat16)
                low = (mean - high.astype(jnp.float32)).astype(jnp.bfloat16)
                value = value_up_ref[:, h * VD : (h + 1) * VD]
                out_ref[i, :rows, h * VD : (h + 1) * VD] = (
                    jnp.dot(high, value, preferred_element_type=jnp.float32)
                    + jnp.dot(low, value, preferred_element_type=jnp.float32)
                ).astype(out_ref.dtype)
                level = jnp.where(seen, max_ref[at] + jnp.log2(total), -HUGE).T[:1]
                for term in range(3):
                    rounded = level.astype(jnp.bfloat16)
                    out_ref[i, pl.ds(rows + h * 3 + term, 1), :] = rounded
                    level = level - rounded.astype(jnp.float32)


def attend(place, mine, other, queries, key_up, value_up, gain, block_tables, near, far):
    count, rows, _ = queries.shape
    heads = key_up.shape[0] // NOPE

    def whole(*shape):
        return pl.BlockSpec(shape, lambda i, w: (0,) * len(shape))

    keys = pl.BlockSpec((4, Y, 80, HALF), lambda i, w: (0, i, 0, 0))
    table = pl.BlockSpec((Y, ROPE // 2, 1), lambda i, w: (w[i], 0, 0))
    return pl.pallas_call(
        attend_kernel,
        out_shape=jax.ShapeDtypeStruct((count, rows + EXTRA, heads * VD), jnp.bfloat16),
        grid_spec=pltpu.PrefetchScalarGridSpec(
            num_scalar_prefetch=1,
            grid=(2,),
            in_specs=[
                keys,
                keys,
                whole(*queries.shape),
                whole(*key_up.shape),
                whole(*value_up.shape),
                whole(ROPE, 1),
                table,
                table,
                whole(*near.shape),
                whole(*far.shape),
            ],
            out_specs=whole(count, rows + EXTRA, heads * VD),
            scratch_shapes=[
                pltpu.VMEM((count * heads, rows, 128), jnp.float32),
                pltpu.VMEM((count * heads, rows, 128), jnp.float32),
                pltpu.VMEM((count * heads, rows, 256), jnp.float32),
                pltpu.VMEM((heads, 256, Y * rows), jnp.bfloat16),
                pltpu.VMEM((256, Y * rows), jnp.bfloat16),
            ],
        ),
        compiler_params=pltpu.CompilerParams(
            dimension_semantics=("arbitrary",), vmem_limit_bytes=60 * 2**20
        ),
        cost_estimate=pl.CostEstimate(
            flops=5 * 2 * rows * Y * rows * heads * 512,
            bytes_accessed=mine.size * 4,
            transcendentals=5 * rows * Y * rows * heads,
        ),
        name="attend",
    )(place, mine, other, queries, key_up, value_up, gain, *block_tables, near, far)


def to_all(value, axis, groups=None):
    count = len(groups[0]) if groups else lax.axis_size(axis)
    return lax.all_to_all(
        jnp.broadcast_to(value[None], (count, *value.shape)), axis, 0, 0, axis_index_groups=groups
    )


def local(
    q_latent,
    kv_latent,
    key_rope,
    pool_input,
    q_lat_gain,
    kv_lat_gain,
    q_head_gain,
    k_head_gain,
    pool_gain,
    q_up,
    key_up,
    value_up,
    pool_mix,
    out_pool,
    out_attn,
):
    row_count = q_latent.shape[0]
    sp_index = lax.axis_index("sp")
    sp_size = lax.axis_size("sp")
    core = lax.axis_index("tp")
    line = lax.axis_index("fs")
    z, y = sp_index // Y, sp_index % Y
    own_pos = sp_index * row_count + jnp.arange(row_count, dtype=jnp.int32)
    key_groups = [
        [p * Y + n for p in (j, PLANES - 1 - j) for n in range(Y)] for j in range(PLANES // 2)
    ]
    query_groups = [
        [(c + 2 * i) * Y + n for i in range(MEMBERS)] for c in range(2) for n in range(Y)
    ]
    block_cos, block_sin, in_cos, in_sin = turn_tables(row_count, sp_size)

    share = lax.dynamic_slice_in_dim(kv_latent, core * HALF, HALF, 0)
    share_rope = lax.dynamic_slice_in_dim(key_rope, core * HALF, HALF, 0)
    share = row_norm(share.astype(jnp.float32), kv_lat_gain).astype(jnp.bfloat16)
    share = jnp.concatenate([share.T, share_rope.T], axis=0)
    share = lax.dynamic_slice_in_dim(share, line * 80, 80, 0)
    mine = to_all(to_all(share, "sp", key_groups), "fs")
    other = lax.ppermute(mine, "tp", [(0, 1), (1, 0)])

    own_cos = lax.dynamic_slice_in_dim(jnp.asarray(block_cos), sp_index, 1, 0)
    own_sin = lax.dynamic_slice_in_dim(jnp.asarray(block_sin), sp_index, 1, 0)
    queries = make_queries(
        q_latent,
        q_lat_gain,
        q_up,
        q_head_gain,
        k_head_gain,
        own_cos * in_cos - own_sin * in_sin,
        own_sin * in_cos + own_cos * in_sin,
    )
    queries = to_all(queries, "sp", query_groups)
    within = jnp.asarray(np.stack([in_cos.T, in_sin.T]))
    near = lax.dynamic_slice_in_dim(within, core * HALF, HALF, 2)
    far = lax.dynamic_slice_in_dim(within, HALF - core * HALF, HALF, 2)
    low_plane = jnp.minimum(z, PLANES - 1 - z)
    place = jnp.stack([low_plane, PLANES - 1 - low_plane, z % 2, y, core * HALF]).astype(jnp.int32)
    partial_out = attend(
        place,
        mine,
        other,
        queries,
        key_up.T,
        value_up,
        k_head_gain[NOPE:, None],
        [jnp.asarray(t[:, :, None]) for t in (block_cos, block_sin)],
        near,
        far,
    )
    parts = lax.all_to_all(partial_out, "sp", 0, 0, axis_index_groups=query_groups)
    head_count = parts.shape[2] // VD
    terms = parts[:, row_count : row_count + 3 * head_count].astype(jnp.float32)
    level = jnp.sum(terms.reshape(MEMBERS, head_count, 3, row_count), axis=2)
    top = jnp.max(level, axis=0)
    shares = jnp.exp2(level - top)
    total = jnp.sum(shares, axis=0)
    log_weight = (top + jnp.log2(total)) * LN2
    shares = jnp.transpose(shares / total, (0, 2, 1))[..., None]
    attended = jnp.sum(
        parts[:, :row_count].reshape(MEMBERS, row_count, head_count, VD).astype(jnp.float32)
        * shares,
        axis=0,
    )
    attended = attended.reshape(row_count, head_count * VD).astype(jnp.bfloat16)

    earlier = lax.ppermute(
        pool_input[row_count - 15 :], "sp", [(i, i + 1) for i in range(sp_size - 1)]
    )
    extended = jnp.concatenate([earlier, pool_input], axis=0).astype(jnp.float32)
    window = jnp.left_shift(jnp.int32(2), line)
    window_sum = jnp.zeros((row_count, pool_input.shape[1]), jnp.float32)
    for lag_rows in range(16):
        window_sum = window_sum + jnp.where(
            lag_rows < window, extended[15 - lag_rows : 15 - lag_rows + row_count], 0.0
        )
    counts = jnp.minimum(own_pos + 1, window).astype(jnp.float32)[:, None]
    pool_diff = (window_sum / counts - extended[15:]).astype(jnp.bfloat16)
    pooled = (
        jnp.dot(pool_diff, pool_mix[0], preferred_element_type=jnp.float32) * pool_gain
    ).astype(jnp.bfloat16)

    lines = lax.axis_size("fs")
    channels = jnp.concatenate([pooled, attended], axis=1).reshape(lines, 2, -1, 128 + head_count * VD)

    def projected(rows):
        rows = rows.reshape(-1, rows.shape[-1])
        return jnp.dot(rows[:, :128], out_pool, preferred_element_type=jnp.float32) + jnp.dot(
            rows[:, 128:], out_attn, preferred_element_type=jnp.float32
        )

    sent = projected(lax.dynamic_index_in_dim(channels, 1 - core, 1, False)).astype(jnp.bfloat16)
    received = lax.ppermute(sent, "tp", [(0, 1), (1, 0)])
    kept = projected(lax.dynamic_index_in_dim(channels, core, 1, False))
    chip = (kept + received.astype(jnp.float32)).astype(jnp.bfloat16)
    chip = lax.all_to_all(chip.reshape(lines, -1, chip.shape[1]), "fs", 0, 0)
    mixed = jnp.sum(chip.astype(jnp.float32), axis=0).astype(jnp.bfloat16)
    return (mixed, log_weight)


def solution(mesh):
    in_specs = (
        P("sp", None),
        P("sp", None),
        P("sp", None),
        P("sp", "fs"),
        P(),
        P(),
        P(),
        P(),
        P(("fs", "tp")),
        P(None, ("fs", "tp")),
        P(None, ("fs", "tp")),
        P(None, ("fs", "tp")),
        P("fs", None, "tp"),
        P(("fs", "tp"), None),
        P(("fs", "tp"), None),
    )
    out_specs = (P(("sp", "fs", "tp"), None), P(("fs", "tp"), "sp"))
    return jax.shard_map(local, mesh=mesh, in_specs=in_specs, out_specs=out_specs, check_vma=False)
```

```python
import math

import jax
import jax.numpy as jnp
import numpy as np
from jax import lax
from jax.experimental import pallas as pl
from jax.experimental.pallas import tpu as pltpu
from jax.sharding import PartitionSpec as P


NOPE = 128
ROPE = 64
VD = 128
EPS = 1e-06
THETA = 10000.0
HUGE = 1e30
LOG2E = math.log2(math.e)
LN2 = math.log(2.0)
HALF = 128
Y = 8
PLANES = 8
MEMBERS = 4
EXTRA = 16


def turn_tables(block_rows, blocks):
    frequency = 1.0 / THETA ** (np.arange(0, ROPE, 2, dtype=np.float64) / ROPE)
    at_block = (np.arange(blocks) * block_rows)[:, None] * frequency
    within = np.arange(block_rows)[:, None] * frequency
    return [t.astype(np.float32) for a in (at_block, within) for t in (np.cos(a), np.sin(a))]


def row_norm(values, row_gain):
    mean_sq = jnp.mean(values * values, axis=-1, keepdims=True)
    return values * lax.rsqrt(mean_sq + EPS) * row_gain


def make_queries(latent, lat_gain, q_up, norm_gain, key_gain, cosine, sine):
    row_count = latent.shape[0]
    normed = row_norm(latent.astype(jnp.float32), lat_gain).astype(jnp.bfloat16)
    query = jnp.dot(normed, q_up, preferred_element_type=jnp.float32).reshape(
        row_count, -1, NOPE + ROPE
    )
    query = row_norm(query, norm_gain)
    scale = LOG2E * (NOPE + ROPE) ** (-0.5)
    cosine, sine = cosine[:, None, :] * scale, sine[:, None, :] * scale
    a, b = query[..., NOPE : NOPE + ROPE // 2], query[..., NOPE + ROPE // 2 :]
    turned = jnp.concatenate([a * cosine - b * sine, a * sine + b * cosine], axis=-1)
    return jnp.concatenate(
        [
            (query[..., :NOPE] * (key_gain[:NOPE] * scale)).reshape(row_count, -1),
            turned.reshape(row_count, -1),
        ],
        axis=-1,
    ).astype(jnp.bfloat16)


def attend_kernel(
    place_ref,
    mine_ref,
    other_ref,
    *refs,
):
    query_refs, refs = refs[:MEMBERS], refs[MEMBERS:]
    (
        key_up_ref,
        value_up_ref,
        gain_ref,
        block_cos_ref,
        block_sin_ref,
        near_ref,
        far_ref,
        out_ref,
        q_ref,
        lat_ref,
        weight_ref,
        *refs,
    ) = refs
    heads = key_up_ref.shape[0] // NOPE
    max_refs, sum_refs, acc_refs, key_refs, score_refs = (
        refs[n * heads : (n + 1) * heads] for n in range(5)
    )
    count = MEMBERS
    rows = query_refs[0].shape[0]
    step = pl.program_id(0)
    plane, parity, own_y = place_ref[step], place_ref[2], place_ref[3]
    offset, member = place_ref[4], place_ref[5]
    width = Y * rows

    @pl.when(step == 0)
    def _():
        for d in range(count):
            q_ref[lax.rem(member + (count - d), count)] = query_refs[d][...]
        for h in range(heads):
            max_refs[h][...] = jnp.full(max_refs[h].shape, -HUGE, jnp.float32)
            sum_refs[h][...] = jnp.zeros_like(sum_refs[h])
            acc_refs[h][...] = jnp.zeros_like(acc_refs[h])
            key_refs[h][NOPE:, :] = jnp.zeros((256 - NOPE, width), jnp.bfloat16)

    def build_keys():
        @pl.loop(0, Y)
        def _(n):
            for u, (keys_ref, in_ref) in enumerate(((mine_ref, near_ref), (other_ref, far_ref))):
                in_cos, in_sin = in_ref[0], in_ref[1]
                at = pl.ds(pl.multiple_of((u * Y + n) * HALF, HALF), HALF)
                parts = [keys_ref[x, n] for x in range(4)]
                latent = jnp.concatenate([*parts[:3], parts[3][:16]], axis=0)
                lat_ref[:, at] = latent
                raw = jnp.dot(key_up_ref[...], latent, preferred_element_type=jnp.float32)
                rope = parts[3][16:].astype(jnp.float32)
                rope_sq = jnp.sum(rope * rope, axis=0, keepdims=True)
                rope = rope * gain_ref[...]
                block_cos, block_sin = block_cos_ref[n], block_sin_ref[n]
                cosine = block_cos * in_cos - block_sin * in_sin
                sine = block_sin * in_cos + block_cos * in_sin
                a, b = rope[: ROPE // 2], rope[ROPE // 2 :]
                turned = jnp.concatenate([a * cosine - b * sine, a * sine + b * cosine], axis=0)
                for h in range(heads):
                    part = raw[h * NOPE : (h + 1) * NOPE]
                    square = jnp.sum(part * part, axis=0, keepdims=True) + rope_sq
                    inverse = lax.rsqrt(square * (1.0 / (NOPE + ROPE)) + EPS)
                    key_refs[h][:NOPE, at] = (part * inverse).astype(jnp.bfloat16)
                    key_refs[h][NOPE + h * ROPE : NOPE + (h + 1) * ROPE, at] = (
                        turned * inverse
                    ).astype(jnp.bfloat16)

    def score(i, h):
        query = jnp.concatenate(
            [q_ref[i, :, h * NOPE : (h + 1) * NOPE], q_ref[i, :, heads * NOPE :]], axis=1
        )
        score_refs[h][...] = jnp.dot(query, key_refs[h][...], preferred_element_type=jnp.float32)

    def mask(h):
        column = lax.broadcasted_iota(jnp.int32, (rows, width), 1)
        row = lax.broadcasted_iota(jnp.int32, (rows, width), 0)
        half_at = jnp.where(column < Y * HALF, offset, HALF - offset)
        key_at = (column % (Y * HALF)) // HALF * rows + half_at + column % HALF
        seen = key_at <= own_y * rows + row
        score_refs[h][...] = jnp.where(seen, score_refs[h][...], -HUGE)

    def weigh(i, h):
        slices = [pl.ds(n * 128, 128) for n in range(width // 128)]
        top = score_refs[h][:, slices[0]]
        for at in slices[1:]:
            top = jnp.maximum(top, score_refs[h][:, at])
        before = max_refs[h][i]
        after = jnp.maximum(before, jnp.max(top, axis=1, keepdims=True))
        factor = jnp.exp2(before - after)
        total = sum_refs[h][i] * factor
        for at in slices:
            weights = jnp.exp2(score_refs[h][:, at] - after)
            weight_ref[:, at] = weights.astype(jnp.bfloat16)
            total = total + weights
        max_refs[h][i] = after
        sum_refs[h][i] = total
        update = lax.dot_general(
            weight_ref[...],
            lat_ref[...],
            (((1,), (1,)), ((), ())),
            preferred_element_type=jnp.float32,
        )
        acc_refs[h][i] = acc_refs[h][i] * jnp.concatenate([factor, factor], axis=1) + update

    first = lax.div(plane - parity + 1, 2)

    @pl.when(first < count)
    def _():
        build_keys()
        score(first, 0)
        own = plane == parity + 2 * first

        @pl.when(own)
        def _():
            for h in range(1, heads):
                score(first, h)
            for h in range(heads):
                mask(h)
            for h in range(heads):
                weigh(first, h)
            score(jnp.minimum(first + 1, count - 1), 0)

        @pl.loop(jnp.where(own, first + 1, first), count)
        def _(i):
            for h in range(heads):
                if h + 1 < heads:
                    score(i, h + 1)
                else:
                    score(jnp.minimum(i + 1, count - 1), 0)
                weigh(i, h)

    @pl.when(step == pl.num_programs(0) - 1)
    def _():
        @pl.loop(0, count)
        def _(i):
            out_ref[i, rows:, :] = jnp.zeros((EXTRA, heads * VD), out_ref.dtype)
            for h in range(heads):
                total = jnp.sum(sum_refs[h][i], axis=1, keepdims=True)
                seen = total > 0.0
                total = jnp.where(seen, total, 1.0)
                mean = acc_refs[h][i] / total
                high = mean.astype(jnp.bfloat16)
                low = (mean - high.astype(jnp.float32)).astype(jnp.bfloat16)
                value = value_up_ref[:, h * VD : (h + 1) * VD]
                out_ref[i, :rows, h * VD : (h + 1) * VD] = (
                    jnp.dot(high, value, preferred_element_type=jnp.float32)
                    + jnp.dot(low, value, preferred_element_type=jnp.float32)
                ).astype(out_ref.dtype)
                level = jnp.where(seen, max_refs[h][i] + jnp.log2(total), -HUGE).T[:1]
                for term in range(3):
                    rounded = level.astype(jnp.bfloat16)
                    out_ref[i, pl.ds(rows + h * 3 + term, 1), :] = rounded
                    level = level - rounded.astype(jnp.float32)


def attend(place, mine, other, queries, key_up, value_up, gain, block_tables, near, far):
    rows, channels = queries[0].shape
    heads = key_up.shape[0] // NOPE

    def whole(*shape):
        return pl.BlockSpec(shape, lambda i, w: (0,) * len(shape))

    keys = pl.BlockSpec((4, Y, 80, HALF), lambda i, w: (0, i, 0, 0))
    table = pl.BlockSpec((Y, ROPE // 2, 1), lambda i, w: (w[i], 0, 0))
    wide = [
        pltpu.VMEM((MEMBERS, rows, 128), jnp.float32),
        pltpu.VMEM((MEMBERS, rows, 128), jnp.float32),
        pltpu.VMEM((MEMBERS, rows, 256), jnp.float32),
        pltpu.VMEM((256, Y * rows), jnp.bfloat16),
        pltpu.VMEM((rows, Y * rows), jnp.float32),
    ]
    return pl.pallas_call(
        attend_kernel,
        out_shape=jax.ShapeDtypeStruct((MEMBERS, rows + EXTRA, heads * VD), jnp.bfloat16),
        grid_spec=pltpu.PrefetchScalarGridSpec(
            num_scalar_prefetch=1,
            grid=(2,),
            in_specs=[
                keys,
                keys,
                *[whole(rows, channels)] * MEMBERS,
                whole(*key_up.shape),
                whole(*value_up.shape),
                whole(ROPE, 1),
                table,
                table,
                whole(*near.shape),
                whole(*far.shape),
            ],
            out_specs=whole(MEMBERS, rows + EXTRA, heads * VD),
            scratch_shapes=[
                pltpu.VMEM((MEMBERS, rows, channels), jnp.bfloat16),
                pltpu.VMEM((256, Y * rows), jnp.bfloat16),
                pltpu.VMEM((rows, Y * rows), jnp.bfloat16),
                *[s for s in wide for _ in range(heads)],
            ],
        ),
        compiler_params=pltpu.CompilerParams(
            dimension_semantics=("arbitrary",), vmem_limit_bytes=60 * 2**20
        ),
        cost_estimate=pl.CostEstimate(
            flops=5 * 2 * rows * Y * rows * heads * 512,
            bytes_accessed=mine.size * 4,
            transcendentals=5 * rows * Y * rows * heads,
        ),
        name="attend",
    )(place, mine, other, *queries, key_up, value_up, gain, *block_tables, near, far)


def to_all(value, axis, groups=None):
    count = len(groups[0]) if groups else lax.axis_size(axis)
    return lax.all_to_all(
        jnp.broadcast_to(value[None], (count, *value.shape)), axis, 0, 0, axis_index_groups=groups
    )


def local(
    q_latent,
    kv_latent,
    key_rope,
    pool_input,
    q_lat_gain,
    kv_lat_gain,
    q_head_gain,
    k_head_gain,
    pool_gain,
    q_up,
    key_up,
    value_up,
    pool_mix,
    out_pool,
    out_attn,
):
    row_count = q_latent.shape[0]
    sp_index = lax.axis_index("sp")
    sp_size = lax.axis_size("sp")
    core = lax.axis_index("tp")
    line = lax.axis_index("fs")
    z, y = lax.div(sp_index, Y), lax.rem(sp_index, Y)
    own_pos = sp_index * row_count + jnp.arange(row_count, dtype=jnp.int32)
    key_groups = [
        [p * Y + n for p in (j, PLANES - 1 - j) for n in range(Y)] for j in range(PLANES // 2)
    ]
    query_groups = [
        [(c + 2 * i) * Y + n for i in range(MEMBERS)] for c in range(2) for n in range(Y)
    ]
    block_cos, block_sin, in_cos, in_sin = turn_tables(row_count, sp_size)

    share = lax.dynamic_slice_in_dim(kv_latent, core * HALF, HALF, 0)
    share_rope = lax.dynamic_slice_in_dim(key_rope, core * HALF, HALF, 0)
    share = row_norm(share.astype(jnp.float32), kv_lat_gain).astype(jnp.bfloat16)
    share = jnp.concatenate([share.T, share_rope.T], axis=0)
    share = lax.dynamic_slice_in_dim(share, line * 80, 80, 0)
    mine = to_all(share, "sp", key_groups)
    mine = to_all(mine, "fs")
    other = lax.ppermute(mine, "tp", [(0, 1), (1, 0)])

    own_cos = lax.dynamic_slice_in_dim(jnp.asarray(block_cos), sp_index, 1, 0)
    own_sin = lax.dynamic_slice_in_dim(jnp.asarray(block_sin), sp_index, 1, 0)
    queries = make_queries(
        q_latent,
        q_lat_gain,
        q_up,
        q_head_gain,
        k_head_gain,
        own_cos * in_cos - own_sin * in_sin,
        own_sin * in_cos + own_cos * in_sin,
    )
    queries = [queries] + [
        lax.ppermute(
            queries,
            "sp",
            [(g[i], g[(i + d) % MEMBERS]) for g in query_groups for i in range(MEMBERS)],
        )
        for d in range(1, MEMBERS)
    ]
    within = jnp.asarray(np.stack([in_cos.T, in_sin.T]))
    near = lax.dynamic_slice_in_dim(within, core * HALF, HALF, 2)
    far = lax.dynamic_slice_in_dim(within, HALF - core * HALF, HALF, 2)
    low_plane = jnp.minimum(z, PLANES - 1 - z)
    place = jnp.stack(
        [low_plane, PLANES - 1 - low_plane, lax.rem(z, 2), y, core * HALF, lax.div(z, 2)]
    ).astype(jnp.int32)
    partial_out = attend(
        place,
        mine,
        other,
        queries,
        key_up.T,
        value_up,
        k_head_gain[NOPE:, None],
        [jnp.asarray(t[:, :, None]) for t in (block_cos, block_sin)],
        near,
        far,
    )
    parts = lax.all_to_all(partial_out, "sp", 0, 0, axis_index_groups=query_groups)
    head_count = parts.shape[2] // VD
    terms = parts[:, row_count : row_count + 3 * head_count].astype(jnp.float32)
    level = jnp.sum(terms.reshape(MEMBERS, head_count, 3, row_count), axis=2)
    top = jnp.max(level, axis=0)
    shares = jnp.exp2(level - top)
    total = jnp.sum(shares, axis=0)
    log_weight = (top + jnp.log2(total)) * LN2
    shares = jnp.transpose(shares / total, (0, 2, 1))[..., None]
    attended = jnp.sum(
        parts[:, :row_count].reshape(MEMBERS, row_count, head_count, VD).astype(jnp.float32)
        * shares,
        axis=0,
    )
    attended = attended.reshape(row_count, head_count * VD).astype(jnp.bfloat16)

    earlier = lax.ppermute(
        pool_input[row_count - 15 :], "sp", [(i, i + 1) for i in range(sp_size - 1)]
    )
    extended = jnp.concatenate([earlier, pool_input], axis=0).astype(jnp.float32)
    window = jnp.left_shift(jnp.int32(2), line)
    window_sum = jnp.zeros((row_count, pool_input.shape[1]), jnp.float32)
    for lag_rows in range(16):
        window_sum = window_sum + jnp.where(
            lag_rows < window, extended[15 - lag_rows : 15 - lag_rows + row_count], 0.0
        )
    counts = jnp.minimum(own_pos + 1, window).astype(jnp.float32)[:, None]
    pool_diff = (window_sum / counts - extended[15:]).astype(jnp.bfloat16)
    pooled = (
        jnp.dot(pool_diff, pool_mix[0], preferred_element_type=jnp.float32) * pool_gain
    ).astype(jnp.bfloat16)

    lines = lax.axis_size("fs")
    channels = jnp.concatenate([pooled, attended], axis=1).reshape(lines, 2, -1, 128 + head_count * VD)

    def projected(rows):
        rows = rows.reshape(-1, rows.shape[-1])
        return jnp.dot(rows[:, :128], out_pool, preferred_element_type=jnp.float32) + jnp.dot(
            rows[:, 128:], out_attn, preferred_element_type=jnp.float32
        )

    sent = projected(lax.dynamic_index_in_dim(channels, 1 - core, 1, False)).astype(jnp.bfloat16)
    received = lax.ppermute(sent, "tp", [(0, 1), (1, 0)])
    kept = projected(lax.dynamic_index_in_dim(channels, core, 1, False))
    chip = (kept + received.astype(jnp.float32)).astype(jnp.bfloat16)
    chip = lax.all_to_all(chip.reshape(lines, -1, chip.shape[1]), "fs", 0, 0)
    mixed = jnp.sum(chip.astype(jnp.float32), axis=0).astype(jnp.bfloat16)
    return (mixed, log_weight)


def solution(mesh):
    in_specs = (
        P("sp", None),
        P("sp", None),
        P("sp", None),
        P("sp", "fs"),
        P(),
        P(),
        P(),
        P(),
        P(("fs", "tp")),
        P(None, ("fs", "tp")),
        P(None, ("fs", "tp")),
        P(None, ("fs", "tp")),
        P("fs", None, "tp"),
        P(("fs", "tp"), None),
        P(("fs", "tp"), None),
    )
    out_specs = (P(("sp", "fs", "tp"), None), P(("fs", "tp"), "sp"))

    return jax.shard_map(local, mesh=mesh, in_specs=in_specs, out_specs=out_specs, check_vma=False)
```

```python
import math

import jax
import jax.numpy as jnp
import numpy as np
from jax import lax
from jax.experimental import pallas as pl
from jax.experimental.pallas import tpu as pltpu
from jax.sharding import PartitionSpec as P


NOPE = 128
ROPE = 64
VD = 128
EPS = 1e-06
THETA = 10000.0
HUGE = 1e30
LOG2E = math.log2(math.e)
LN2 = math.log(2.0)
HALF = 128
Y = 8
PLANES = 8
MEMBERS = 4
VMEM_LIMIT = 32 * 2**20
EXTRA = 16


def turn_tables(block_rows, blocks):
    frequency = 1.0 / THETA ** (np.arange(0, ROPE, 2, dtype=np.float64) / ROPE)
    at_block = (np.arange(blocks) * block_rows)[:, None] * frequency
    within = np.arange(block_rows)[:, None] * frequency
    return [t.astype(np.float32) for a in (at_block, within) for t in (np.cos(a), np.sin(a))]


def row_norm(values, row_gain):
    mean_sq = jnp.mean(values * values, axis=-1, keepdims=True)
    return values * lax.rsqrt(mean_sq + EPS) * row_gain


def make_queries(latent, lat_gain, q_up, norm_gain, key_gain, cosine, sine):
    row_count = latent.shape[0]
    normed = row_norm(latent.astype(jnp.float32), lat_gain).astype(jnp.bfloat16)
    query = jnp.dot(normed, q_up, preferred_element_type=jnp.float32).reshape(
        row_count, -1, NOPE + ROPE
    )
    query = row_norm(query, norm_gain)
    scale = LOG2E * (NOPE + ROPE) ** (-0.5)
    cosine, sine = cosine[:, None, :] * scale, sine[:, None, :] * scale
    a, b = query[..., NOPE : NOPE + ROPE // 2], query[..., NOPE + ROPE // 2 :]
    turned = jnp.concatenate([a * cosine - b * sine, a * sine + b * cosine], axis=-1)
    return jnp.concatenate(
        [
            (query[..., :NOPE] * (key_gain[:NOPE] * scale)).reshape(row_count, -1),
            turned.reshape(row_count, -1),
        ],
        axis=-1,
    ).astype(jnp.bfloat16)


def attend_kernel(place_ref, mine_ref, other_ref, *refs):
    query_refs, refs = refs[:MEMBERS], refs[MEMBERS:]
    key_up_ref, value_up_ref, gain_ref, block_ref, near_ref, far_ref, out_ref, *refs = refs
    q_ref, lat_ref, weight_ref, turn_ref, up_ref, *refs = refs
    heads = key_up_ref.shape[1] // NOPE
    max_refs, sum_refs, acc_refs, key_refs, score_refs, top_refs = (
        refs[n * heads : (n + 1) * heads] for n in range(6)
    )
    count = MEMBERS
    rows = query_refs[0].shape[0]
    parity, own_y, offset, member = place_ref[2], place_ref[3], place_ref[4], place_ref[5]
    width = Y * rows
    slices = [pl.ds(n * 128, 128) for n in range(width // 128)]
    chunk = min(4, Y) * HALF

    for d in range(count):
        q_ref[lax.rem(member + (count - d), count)] = query_refs[d][...]
    for h in range(heads):
        max_refs[h][...] = jnp.full(max_refs[h].shape, -HUGE, jnp.float32)
        sum_refs[h][...] = jnp.zeros_like(sum_refs[h])
        acc_refs[h][...] = jnp.zeros_like(acc_refs[h])
        key_refs[h][NOPE:, :] = jnp.zeros((256 - NOPE, width), jnp.bfloat16)
    up_ref[...] = key_up_ref[...].T
    gain = jnp.broadcast_to(gain_ref[:, NOPE:], (ROPE, ROPE)).T[:, :1]

    def build_keys(step, plane):
        for u, (keys_ref, in_ref) in enumerate(((mine_ref, near_ref), (other_ref, far_ref))):
            for n in range(Y):
                at = pl.ds((u * Y + n) * HALF, HALF)
                for x in range(4):
                    part = keys_ref[x, step * Y + n]
                    if x < 3:
                        lat_ref[x * 80 : (x + 1) * 80, at] = part
                    else:
                        lat_ref[240:256, at] = part[:16]
                        turn_ref[:, at] = part[16:].astype(jnp.float32)

        def turn(u, in_ref):
            for n in range(Y):
                at = pl.ds((u * Y + n) * HALF, HALF)
                in_cos, in_sin = in_ref[0], in_ref[1]
                block_cos = block_ref[plane, : ROPE // 2, n : n + 1]
                block_sin = block_ref[plane, ROPE // 2 :, n : n + 1]
                cosine = block_cos * in_cos - block_sin * in_sin
                sine = block_sin * in_cos + block_cos * in_sin
                raw = turn_ref[:, at]
                square = jnp.sum(raw * raw, axis=0, keepdims=True)
                raw = raw * gain
                a, b = raw[: ROPE // 2], raw[ROPE // 2 :]
                turn_ref[: ROPE // 2, at] = a * cosine - b * sine
                turn_ref[ROPE // 2 :, at] = a * sine + b * cosine
                top_refs[0][n : n + 1, u * 128 : (u + 1) * 128] = square

        for u, in_ref in enumerate((near_ref, far_ref)):
            turn(u, in_ref)
        for n in range(width // chunk):
            at = pl.ds(n * chunk, chunk)
            raw = jnp.dot(up_ref[...], lat_ref[:, at], preferred_element_type=jnp.float32)
            u, first = n * chunk // (Y * HALF), n * chunk % (Y * HALF) // HALF
            rope_sq = jnp.concatenate(
                [top_refs[0][k : k + 1, u * 128 : (u + 1) * 128] for k in range(first, first + chunk // HALF)],
                axis=1,
            )
            for h in range(heads):
                part = raw[h * NOPE : (h + 1) * NOPE]
                square = jnp.sum(part * part, axis=0, keepdims=True) + rope_sq
                inverse = lax.rsqrt(square * (1.0 / (NOPE + ROPE)) + EPS)
                key_refs[h][:NOPE, at] = (part * inverse).astype(jnp.bfloat16)
                key_refs[h][NOPE + h * ROPE : NOPE + (h + 1) * ROPE, at] = (
                    turn_ref[:, at] * inverse
                ).astype(jnp.bfloat16)

    def score(i, h):
        query = jnp.concatenate(
            [q_ref[i, :, h * NOPE : (h + 1) * NOPE], q_ref[i, :, heads * NOPE :]], axis=1
        )
        scores = jnp.dot(query, key_refs[h][...], preferred_element_type=jnp.float32)
        score_refs[h][...] = scores
        top = scores[:, :128]
        for n in range(1, width // 128):
            top = jnp.maximum(top, scores[:, n * 128 : (n + 1) * 128])
        top_refs[h][:, :128] = top

    def mask(h):
        column = lax.broadcasted_iota(jnp.int32, (rows, width), 1)
        row = lax.broadcasted_iota(jnp.int32, (rows, width), 0)
        half_at = jnp.where(column < Y * HALF, offset, HALF - offset)
        key_at = (column % (Y * HALF)) // HALF * rows + half_at + column % HALF
        seen = key_at <= own_y * rows + row
        scores = jnp.where(seen, score_refs[h][...], -HUGE)
        score_refs[h][...] = scores
        top = scores[:, :128]
        for n in range(1, width // 128):
            top = jnp.maximum(top, scores[:, n * 128 : (n + 1) * 128])
        top_refs[h][:, :128] = top

    def weigh(i, h):
        before = max_refs[h][i]
        after = jnp.maximum(before, jnp.max(top_refs[h][:, :128], axis=1, keepdims=True))
        factor = jnp.exp2(before - after)
        total = sum_refs[h][i] * factor
        for at in slices:
            weights = jnp.exp2(score_refs[h][:, at] - after)
            weight_ref[:, at] = weights.astype(jnp.bfloat16)
            total = total + weights
        max_refs[h][i] = after
        sum_refs[h][i] = total
        update = lax.dot_general(
            weight_ref[...],
            lat_ref[...],
            (((1,), (1,)), ((), ())),
            preferred_element_type=jnp.float32,
        )
        acc_refs[h][i] = acc_refs[h][i] * jnp.concatenate([factor, factor], axis=1) + update

    @pl.loop(0, 2)
    def _(step):
        plane = place_ref[step]
        first = lax.div(plane - parity + 1, 2)

        @pl.when(first < count)
        def _():
            build_keys(step, plane)
            score(first, 0)
            own = plane == parity + 2 * first

            @pl.when(own)
            def _():
                for h in range(1, heads):
                    score(first, h)
                for h in range(heads):
                    mask(h)
                for h in range(heads):
                    weigh(first, h)
                score(jnp.minimum(first + 1, count - 1), 0)

            @pl.loop(jnp.where(own, first + 1, first), count)
            def _(i):
                for h in range(heads):
                    if h + 1 < heads:
                        score(i, h + 1)
                    else:
                        score(jnp.minimum(i + 1, count - 1), 0)
                    weigh(i, h)

    @pl.loop(0, count)
    def _(i):
        out_ref[i, rows:, :] = jnp.zeros((EXTRA, heads * VD), out_ref.dtype)
        for h in range(heads):
            total = jnp.sum(sum_refs[h][i], axis=1, keepdims=True)
            seen = total > 0.0
            total = jnp.where(seen, total, 1.0)
            mean = (acc_refs[h][i] * (1.0 / total)).astype(jnp.bfloat16)
            out_ref[i, :rows, h * VD : (h + 1) * VD] = jnp.dot(
                mean, value_up_ref[:, h * VD : (h + 1) * VD], preferred_element_type=jnp.float32
            ).astype(out_ref.dtype)
            level = jnp.where(seen, max_refs[h][i] + jnp.log2(total), -HUGE).T[:1]
            for term in range(3):
                rounded = level.astype(jnp.bfloat16)
                out_ref[i, pl.ds(rows + h * 3 + term, 1), :] = rounded
                level = level - rounded.astype(jnp.float32)


def attend(place, mine, other, queries, key_up, value_up, gain, block_table, near, far):
    rows, channels = queries[0].shape
    heads = key_up.shape[1] // NOPE
    vmem = pl.BlockSpec(memory_space=pltpu.VMEM)
    wide = [
        pltpu.VMEM((MEMBERS, rows, 128), jnp.float32),
        pltpu.VMEM((MEMBERS, rows, 128), jnp.float32),
        pltpu.VMEM((MEMBERS, rows, 256), jnp.float32),
        pltpu.VMEM((256, Y * rows), jnp.bfloat16),
        pltpu.VMEM((rows, Y * rows), jnp.float32),
        pltpu.VMEM((rows, 256), jnp.float32),
    ]
    return pl.pallas_call(
        attend_kernel,
        out_shape=jax.ShapeDtypeStruct((MEMBERS, rows + EXTRA, heads * VD), jnp.bfloat16),
        in_specs=[pl.BlockSpec(memory_space=pltpu.SMEM)] + [vmem] * (8 + MEMBERS),
        out_specs=vmem,
        scratch_shapes=[
            pltpu.VMEM((MEMBERS, rows, channels), jnp.bfloat16),
            pltpu.VMEM((256, Y * rows), jnp.bfloat16),
            pltpu.VMEM((rows, Y * rows), jnp.bfloat16),
            pltpu.VMEM((ROPE, Y * rows), jnp.float32),
            pltpu.VMEM(key_up.shape[::-1], jnp.bfloat16),
            *[s for s in wide for _ in range(heads)],
        ],
        compiler_params=pltpu.CompilerParams(vmem_limit_bytes=VMEM_LIMIT),
        cost_estimate=pl.CostEstimate(
            flops=5 * 2 * rows * Y * rows * heads * 512,
            bytes_accessed=mine.size * 4,
            transcendentals=5 * rows * Y * rows * heads,
        ),
        name="attend",
    )(place, mine, other, *queries, key_up, value_up, gain, block_table, near, far)


def share_kernel(place_ref, latent_ref, rope_ref, gain_ref, out_ref, all_ref):
    latent = latent_ref[...].astype(jnp.float32)
    normed = row_norm(latent, gain_ref[...]).astype(jnp.bfloat16)
    all_ref[: latent.shape[1]] = normed.T
    all_ref[latent.shape[1] :] = rope_ref[...].T
    own = all_ref[pl.ds(pl.multiple_of(place_ref[1] * 80, 16), 80), :]
    for n in range(out_ref.shape[0]):
        out_ref[n] = own


def key_share(place, latent, rope, gain, count):
    channels = latent.shape[1] + rope.shape[1]
    return pl.pallas_call(
        share_kernel,
        out_shape=jax.ShapeDtypeStruct((count, 80, HALF), jnp.bfloat16),
        grid_spec=pltpu.PrefetchScalarGridSpec(
            num_scalar_prefetch=1,
            grid=(1,),
            in_specs=[
                pl.BlockSpec((HALF, latent.shape[1]), lambda i, w: (w[0], 0)),
                pl.BlockSpec((HALF, rope.shape[1]), lambda i, w: (w[0], 0)),
                pl.BlockSpec((1, latent.shape[1]), lambda i, w: (0, 0)),
            ],
            out_specs=pl.BlockSpec((count, 80, HALF), lambda i, w: (0, 0, 0)),
            scratch_shapes=[pltpu.VMEM((channels, HALF), jnp.bfloat16)],
        ),
        cost_estimate=pl.CostEstimate(flops=10**6, bytes_accessed=10**6, transcendentals=HALF),
        compiler_params=pltpu.CompilerParams(vmem_limit_bytes=4 * 2**20),
        name="key_share",
    )(place, latent, rope, gain[None])


def merge_kernel(parts_ref, out_ref, log_ref, turn_ref):
    count, rows = parts_ref.shape[0], out_ref.shape[0]
    heads = out_ref.shape[1] // VD
    turn_ref[...] = jnp.zeros_like(turn_ref)
    for h in range(heads):
        levels = []
        for i in range(count):
            terms = [
                parts_ref[i, rows : rows + EXTRA, :].astype(jnp.float32)[h * 3 + k : h * 3 + k + 1]
                for k in range(3)
            ]
            levels.append(terms[0] + terms[1] + terms[2])
        top = levels[0]
        for level in levels[1:]:
            top = jnp.maximum(top, level)
        shares = [jnp.exp2(level - top) for level in levels]
        total = shares[0]
        for share in shares[1:]:
            total = total + share
        log_ref[h : h + 1, :] = (top + jnp.log2(total)) * LN2
        inverse = 1.0 / total
        for i in range(count):
            turn_ref[h * count + i : h * count + i + 1, :] = shares[i] * inverse
    turned = turn_ref[...].T
    for h in range(heads):
        merged = jnp.zeros((rows, VD), jnp.float32)
        for i in range(count):
            k = h * count + i
            part = parts_ref[i, :rows, h * VD : (h + 1) * VD].astype(jnp.float32)
            merged = merged + part * turned[:, k : k + 1]
        out_ref[:, h * VD : (h + 1) * VD] = merged.astype(out_ref.dtype)


def merge(parts):
    _, rows, channels = parts.shape
    rows -= EXTRA
    vmem = pl.BlockSpec(memory_space=pltpu.VMEM)
    return pl.pallas_call(
        merge_kernel,
        out_shape=[
            jax.ShapeDtypeStruct((rows, channels), jnp.bfloat16),
            jax.ShapeDtypeStruct((channels // VD, rows), jnp.float32),
        ],
        in_specs=[vmem],
        out_specs=[vmem, vmem],
        scratch_shapes=[pltpu.VMEM((128, rows), jnp.float32)],
        cost_estimate=pl.CostEstimate(flops=10**6, bytes_accessed=10**6, transcendentals=10**4),
        compiler_params=pltpu.CompilerParams(vmem_limit_bytes=8 * 2**20),
        name="merge",
    )(parts)


def to_all(value, axis):
    count = lax.axis_size(axis)
    return lax.all_to_all(jnp.broadcast_to(value[None], (count, *value.shape)), axis, 0, 0)


def local(
    q_latent,
    kv_latent,
    key_rope,
    pool_input,
    q_lat_gain,
    kv_lat_gain,
    q_head_gain,
    k_head_gain,
    pool_gain,
    q_up,
    key_up,
    value_up,
    pool_mix,
    out_pool,
    out_attn,
):
    row_count = q_latent.shape[0]
    sp_index = lax.axis_index("sp")
    sp_size = lax.axis_size("sp")
    core = lax.axis_index("tp")
    line = lax.axis_index("fs")
    z, y = lax.div(sp_index, Y), lax.rem(sp_index, Y)
    own_pos = sp_index * row_count + jnp.arange(row_count, dtype=jnp.int32)
    key_groups = [
        [p * Y + n for p in (j, PLANES - 1 - j) for n in range(Y)] for j in range(PLANES // 2)
    ]
    query_groups = [
        [(c + 2 * i) * Y + n for i in range(MEMBERS)] for c in range(2) for n in range(Y)
    ]
    block_cos, block_sin, in_cos, in_sin = turn_tables(row_count, sp_size)
    plane_turns = np.transpose(
        np.concatenate([block_cos, block_sin], axis=1).reshape(-1, Y, ROPE), (0, 2, 1)
    )

    share = key_share(
        jnp.stack([core, line]).astype(jnp.int32), kv_latent, key_rope, kv_lat_gain, 2 * Y
    )
    mine = lax.all_to_all(share, "sp", 0, 0, axis_index_groups=key_groups)
    mine = to_all(mine, "fs")
    other = lax.ppermute(mine, "tp", [(0, 1), (1, 0)])

    own_cos = lax.dynamic_slice_in_dim(jnp.asarray(block_cos), sp_index, 1, 0)
    own_sin = lax.dynamic_slice_in_dim(jnp.asarray(block_sin), sp_index, 1, 0)
    queries = make_queries(
        q_latent,
        q_lat_gain,
        q_up,
        q_head_gain,
        k_head_gain,
        own_cos * in_cos - own_sin * in_sin,
        own_sin * in_cos + own_cos * in_sin,
    )

    def turned(d):
        pairs = [(g[i], g[(i + d) % MEMBERS]) for g in query_groups for i in range(MEMBERS)]
        return lax.ppermute(queries, "sp", pairs)

    queries = [queries] + [turned(d) for d in range(1, MEMBERS)]
    within = jnp.asarray(np.stack([in_cos.T, in_sin.T]))
    near = lax.dynamic_slice_in_dim(within, core * HALF, HALF, 2)
    far = lax.dynamic_slice_in_dim(within, HALF - core * HALF, HALF, 2)
    low_plane = jnp.minimum(z, PLANES - 1 - z)
    place = jnp.stack(
        [low_plane, PLANES - 1 - low_plane, lax.rem(z, 2), y, core * HALF, lax.div(z, 2)]
    ).astype(jnp.int32)
    partial_out = attend(
        place,
        mine,
        other,
        queries,
        key_up,
        value_up,
        k_head_gain[None],
        jnp.asarray(plane_turns),
        near,
        far,
    )
    parts = lax.all_to_all(partial_out, "sp", 0, 0, axis_index_groups=query_groups)
    attended, log_weight = merge(parts)

    earlier = lax.ppermute(
        pool_input[row_count - 15 :], "sp", [(i, i + 1) for i in range(sp_size - 1)]
    )
    extended = jnp.concatenate([earlier, pool_input], axis=0).astype(jnp.float32)
    window = jnp.left_shift(jnp.int32(2), line)
    window_sum = jnp.zeros((row_count, pool_input.shape[1]), jnp.float32)
    for lag_rows in range(16):
        window_sum = window_sum + jnp.where(
            lag_rows < window, extended[15 - lag_rows : 15 - lag_rows + row_count], 0.0
        )
    counts = jnp.minimum(own_pos + 1, window).astype(jnp.float32)[:, None]
    pool_diff = (window_sum / counts - extended[15:]).astype(jnp.bfloat16)
    pooled = (
        jnp.dot(pool_diff, pool_mix[0], preferred_element_type=jnp.float32) * pool_gain
    ).astype(jnp.bfloat16)

    lines = lax.axis_size("fs")
    channels = jnp.concatenate([pooled, attended], axis=1).reshape(
        lines, 2, -1, pooled.shape[1] + attended.shape[1]
    )

    def projected(rows):
        rows = rows.reshape(-1, rows.shape[-1])
        return jnp.dot(rows[:, :128], out_pool, preferred_element_type=jnp.float32) + jnp.dot(
            rows[:, 128:], out_attn, preferred_element_type=jnp.float32
        )

    sent = projected(lax.dynamic_index_in_dim(channels, 1 - core, 1, False)).astype(jnp.bfloat16)
    received = lax.ppermute(sent, "tp", [(0, 1), (1, 0)])
    kept = projected(lax.dynamic_index_in_dim(channels, core, 1, False))
    chip = (kept + received.astype(jnp.float32)).astype(jnp.bfloat16)
    chip = lax.all_to_all(chip.reshape(lines, -1, chip.shape[1]), "fs", 0, 0)
    mixed = jnp.sum(chip.astype(jnp.float32), axis=0).astype(jnp.bfloat16)
    return (mixed, log_weight)


def solution(mesh):
    in_specs = (
        P("sp", None),
        P("sp", None),
        P("sp", None),
        P("sp", "fs"),
        P(),
        P(),
        P(),
        P(),
        P(("fs", "tp")),
        P(None, ("fs", "tp")),
        P(None, ("fs", "tp")),
        P(None, ("fs", "tp")),
        P("fs", None, "tp"),
        P(("fs", "tp"), None),
        P(("fs", "tp"), None),
    )
    out_specs = (P(("sp", "fs", "tp"), None), P(("fs", "tp"), "sp"))

    return jax.shard_map(local, mesh=mesh, in_specs=in_specs, out_specs=out_specs, check_vma=False)
```

```python
import math

import jax
import jax.numpy as jnp
import numpy as np
from jax import lax
from jax.experimental import pallas as pl
from jax.experimental.pallas import tpu as pltpu
from jax.sharding import PartitionSpec as P


NOPE = 128
ROPE = 64
VD = 128
EPS = 1e-06
THETA = 10000.0
HUGE = 1e30
LOG2E = math.log2(math.e)
LN2 = math.log(2.0)
HALF = 128
Y = 8
PLANES = 8
MEMBERS = 4
VMEM_LIMIT = 32 * 2**20
EXTRA = 16


def turn_tables(block_rows, blocks):
    frequency = 1.0 / THETA ** (np.arange(0, ROPE, 2, dtype=np.float64) / ROPE)
    at_block = (np.arange(blocks) * block_rows)[:, None] * frequency
    within = np.arange(block_rows)[:, None] * frequency
    return [t.astype(np.float32) for a in (at_block, within) for t in (np.cos(a), np.sin(a))]


def row_norm(values, row_gain):
    mean_sq = jnp.mean(values * values, axis=-1, keepdims=True)
    return values * lax.rsqrt(mean_sq + EPS) * row_gain


def make_queries(latent, lat_gain, q_up, norm_gain, key_gain, cosine, sine):
    row_count = latent.shape[0]
    normed = row_norm(latent.astype(jnp.float32), lat_gain).astype(jnp.bfloat16)
    query = jnp.dot(normed, q_up, preferred_element_type=jnp.float32).reshape(
        row_count, -1, NOPE + ROPE
    )
    query = row_norm(query, norm_gain)
    scale = LOG2E * (NOPE + ROPE) ** (-0.5)
    cosine, sine = cosine[:, None, :] * scale, sine[:, None, :] * scale
    a, b = query[..., NOPE : NOPE + ROPE // 2], query[..., NOPE + ROPE // 2 :]
    turned = jnp.concatenate([a * cosine - b * sine, a * sine + b * cosine], axis=-1)
    return jnp.concatenate(
        [
            (query[..., :NOPE] * (key_gain[:NOPE] * scale)).reshape(row_count, -1),
            turned.reshape(row_count, -1),
        ],
        axis=-1,
    ).astype(jnp.bfloat16)


def attend_kernel(place_ref, mine_ref, other_ref, *refs):
    query_refs, refs = refs[:MEMBERS], refs[MEMBERS:]
    key_up_ref, value_up_ref, gain_ref, block_ref, near_ref, far_ref, out_ref, *refs = refs
    q_ref, lat_ref, turn_ref, up_ref, far_keys_ref, sems, *refs = refs
    heads = key_up_ref.shape[1] // NOPE
    max_refs, sum_refs, acc_refs, key_refs, score_refs, top_refs = (
        refs[n * heads : (n + 1) * heads] for n in range(6)
    )
    count = MEMBERS
    rows = query_refs[0].shape[0]
    parity, own_y, offset, member = place_ref[2], place_ref[3], place_ref[4], place_ref[5]
    width = Y * rows
    slices = [pl.ds(n * 128, 128) for n in range(width // 128)]
    chunk = min(4, Y) * HALF

    arrivals = [
        pltpu.make_async_copy(
            query_refs[d], q_ref.at[lax.rem(member + (count - d), count)], sems.at[d]
        )
        for d in range(count)
    ]
    arrival = pltpu.make_async_copy(other_ref, far_keys_ref, sems.at[count])
    arrival.start()
    for copy in arrivals:
        copy.start()
    for h in range(heads):
        max_refs[h][...] = jnp.full(max_refs[h].shape, -HUGE, jnp.float32)
        sum_refs[h][...] = jnp.zeros_like(sum_refs[h])
        acc_refs[h][...] = jnp.zeros_like(acc_refs[h])
        key_refs[h][NOPE:, :] = jnp.zeros((256 - NOPE, width), jnp.bfloat16)
    up_ref[...] = key_up_ref[...].T
    gain = jnp.broadcast_to(gain_ref[:, NOPE:], (ROPE, ROPE)).T[:, :1]

    def build_keys(step, plane):
        for u, (keys_ref, in_ref) in enumerate(((mine_ref, near_ref), (far_keys_ref, far_ref))):
            in_cos, in_sin = in_ref[0], in_ref[1]
            for n in range(Y):
                at = pl.ds((u * Y + n) * HALF, HALF)
                for x in range(3):
                    lat_ref[x * 80 : (x + 1) * 80, at] = keys_ref[x, step * Y + n]
                last = keys_ref[3, step * Y + n]
                lat_ref[240:256, at] = last[:16]
                raw = last[16:].astype(jnp.float32)
                square = jnp.sum(raw * raw, axis=0, keepdims=True)
                top_refs[0][n : n + 1, u * 128 : (u + 1) * 128] = square
                block_cos = block_ref[plane, : ROPE // 2, n : n + 1]
                block_sin = block_ref[plane, ROPE // 2 :, n : n + 1]
                cosine = block_cos * in_cos - block_sin * in_sin
                sine = block_sin * in_cos + block_cos * in_sin
                raw = raw * gain
                a, b = raw[: ROPE // 2], raw[ROPE // 2 :]
                turn_ref[: ROPE // 2, at] = a * cosine - b * sine
                turn_ref[ROPE // 2 :, at] = a * sine + b * cosine
            for n in range(Y * HALF // chunk):
                at = pl.ds(u * Y * HALF + n * chunk, chunk)
                raw = jnp.dot(up_ref[...], lat_ref[:, at], preferred_element_type=jnp.float32)
                blocks = range(n * chunk // HALF, (n + 1) * chunk // HALF)
                rope_sq = jnp.concatenate(
                    [top_refs[0][k : k + 1, u * 128 : (u + 1) * 128] for k in blocks], axis=1
                )
                for h in range(heads):
                    part = raw[h * NOPE : (h + 1) * NOPE]
                    square = jnp.sum(part * part, axis=0, keepdims=True) + rope_sq
                    inverse = lax.rsqrt(square * (1.0 / (NOPE + ROPE)) + EPS)
                    key_refs[h][:NOPE, at] = (part * inverse).astype(jnp.bfloat16)
                    key_refs[h][NOPE + h * ROPE : NOPE + (h + 1) * ROPE, at] = (
                        turn_ref[:, at] * inverse
                    ).astype(jnp.bfloat16)

    def score(i, h):
        query = jnp.concatenate(
            [q_ref[i, :, h * NOPE : (h + 1) * NOPE], q_ref[i, :, heads * NOPE :]], axis=1
        )
        scores = jnp.dot(query, key_refs[h][...], preferred_element_type=jnp.float32)
        score_refs[h][...] = scores
        top = scores[:, :128]
        for n in range(1, width // 128):
            top = jnp.maximum(top, scores[:, n * 128 : (n + 1) * 128])
        top_refs[h][:, :128] = top

    def mask(h):
        column = lax.broadcasted_iota(jnp.int32, (rows, width), 1)
        row = lax.broadcasted_iota(jnp.int32, (rows, width), 0)
        half_at = jnp.where(column < Y * HALF, offset, HALF - offset)
        key_at = (column % (Y * HALF)) // HALF * rows + half_at + column % HALF
        seen = key_at <= own_y * rows + row
        scores = jnp.where(seen, score_refs[h][...], -HUGE)
        score_refs[h][...] = scores
        top = scores[:, :128]
        for n in range(1, width // 128):
            top = jnp.maximum(top, scores[:, n * 128 : (n + 1) * 128])
        top_refs[h][:, :128] = top

    def weigh(i, h, following=None):
        before = max_refs[h][i]
        after = jnp.maximum(before, jnp.max(top_refs[h][:, :128], axis=1, keepdims=True))
        factor = jnp.exp2(before - after)
        total = sum_refs[h][i] * factor
        update = acc_refs[h][i] * jnp.concatenate([factor, factor], axis=1)
        top = None
        if following is not None:
            j, other = following
            query = jnp.concatenate(
                [q_ref[j, :, other * NOPE : (other + 1) * NOPE], q_ref[j, :, heads * NOPE :]],
                axis=1,
            )
        for n in range(0, len(slices), 4):
            if following is not None:
                at = slice(n * 128, (n + 4) * 128)
                scores = jnp.dot(query, key_refs[other][:, at], preferred_element_type=jnp.float32)
                score_refs[other][:, at] = scores
                for k in range(4):
                    piece = scores[:, k * 128 : (k + 1) * 128]
                    top = piece if top is None else jnp.maximum(top, piece)
            pieces = []
            for at in slices[n : n + 4]:
                weights = jnp.exp2(score_refs[h][:, at] - after)
                pieces.append(weights.astype(jnp.bfloat16))
                total = total + weights
            update = update + lax.dot_general(
                jnp.concatenate(pieces, axis=1),
                lat_ref[:, n * 128 : (n + 4) * 128],
                (((1,), (1,)), ((), ())),
                preferred_element_type=jnp.float32,
            )
        max_refs[h][i] = after
        sum_refs[h][i] = total
        acc_refs[h][i] = update
        if following is not None:
            top_refs[other][:, :128] = top

    arrival.wait()
    for copy in arrivals:
        copy.wait()

    @pl.loop(0, 2)
    def _(step):
        plane = place_ref[step]
        first = lax.div(plane - parity + 1, 2)

        @pl.when(first < count)
        def _():
            build_keys(step, plane)
            score(first, 0)
            own = plane == parity + 2 * first

            @pl.when(own)
            def _():
                for h in range(1, heads):
                    score(first, h)
                for h in range(heads):
                    mask(h)
                for h in range(heads):
                    weigh(first, h)
                score(jnp.minimum(first + 1, count - 1), 0)

            @pl.loop(jnp.where(own, first + 1, first), count)
            def _(i):
                for h in range(heads):
                    if h + 1 < heads:
                        weigh(i, h, (i, h + 1))
                    else:
                        weigh(i, h, (jnp.minimum(i + 1, count - 1), 0))

    @pl.loop(0, count)
    def _(i):
        out_ref[i, rows:, :] = jnp.zeros((EXTRA, heads * VD), out_ref.dtype)
        for h in range(heads):
            total = jnp.sum(sum_refs[h][i], axis=1, keepdims=True)
            seen = total > 0.0
            total = jnp.where(seen, total, 1.0)
            mean = (acc_refs[h][i] * (1.0 / total)).astype(jnp.bfloat16)
            out_ref[i, :rows, h * VD : (h + 1) * VD] = jnp.dot(
                mean, value_up_ref[:, h * VD : (h + 1) * VD], preferred_element_type=jnp.float32
            ).astype(out_ref.dtype)
            level = jnp.where(seen, max_refs[h][i] + jnp.log2(total), -HUGE).T[:1]
            for term in range(3):
                rounded = level.astype(jnp.bfloat16)
                out_ref[i, pl.ds(rows + h * 3 + term, 1), :] = rounded
                level = level - rounded.astype(jnp.float32)


def attend(place, mine, other, queries, key_up, value_up, gain, block_table, near, far):
    rows, channels = queries[0].shape
    heads = key_up.shape[1] // NOPE
    vmem = pl.BlockSpec(memory_space=pltpu.VMEM)
    wide = [
        pltpu.VMEM((MEMBERS, rows, 128), jnp.float32),
        pltpu.VMEM((MEMBERS, rows, 128), jnp.float32),
        pltpu.VMEM((MEMBERS, rows, 256), jnp.float32),
        pltpu.VMEM((256, Y * rows), jnp.bfloat16),
        pltpu.VMEM((rows, Y * rows), jnp.float32),
        pltpu.VMEM((rows, 256), jnp.float32),
    ]
    return pl.pallas_call(
        attend_kernel,
        out_shape=jax.ShapeDtypeStruct((MEMBERS, rows + EXTRA, heads * VD), jnp.bfloat16),
        in_specs=[
            pl.BlockSpec(memory_space=pltpu.SMEM),
            vmem,
            *[pl.BlockSpec(memory_space=pl.ANY)] * (1 + MEMBERS),
            *[vmem] * 6,
        ],
        out_specs=vmem,
        scratch_shapes=[
            pltpu.VMEM((MEMBERS, rows, channels), jnp.bfloat16),
            pltpu.VMEM((256, Y * rows), jnp.bfloat16),
            pltpu.VMEM((ROPE, Y * rows), jnp.float32),
            pltpu.VMEM(key_up.shape[::-1], jnp.bfloat16),
            pltpu.VMEM(other.shape, jnp.bfloat16),
            pltpu.SemaphoreType.DMA((MEMBERS + 1,)),
            *[s for s in wide for _ in range(heads)],
        ],
        compiler_params=pltpu.CompilerParams(vmem_limit_bytes=VMEM_LIMIT),
        cost_estimate=pl.CostEstimate(
            flops=5 * 2 * rows * Y * rows * heads * 512,
            bytes_accessed=mine.size * 4,
            transcendentals=5 * rows * Y * rows * heads,
        ),
        name="attend",
    )(place, mine, other, *queries, key_up, value_up, gain, block_table, near, far)


def share_kernel(place_ref, latent_ref, rope_ref, gain_ref, out_ref, all_ref):
    latent = latent_ref[...].astype(jnp.float32)
    normed = row_norm(latent, gain_ref[...]).astype(jnp.bfloat16)
    all_ref[: latent.shape[1]] = normed.T
    all_ref[latent.shape[1] :] = rope_ref[...]
    own = all_ref[pl.ds(pl.multiple_of(place_ref[1] * 80, 16), 80), :]
    for n in range(out_ref.shape[0]):
        out_ref[n] = own


def key_share(place, latent, rope, gain, count):
    channels = latent.shape[1] + rope.shape[0]
    return pl.pallas_call(
        share_kernel,
        out_shape=jax.ShapeDtypeStruct((count, 80, HALF), jnp.bfloat16),
        grid_spec=pltpu.PrefetchScalarGridSpec(
            num_scalar_prefetch=1,
            grid=(1,),
            in_specs=[
                pl.BlockSpec((HALF, latent.shape[1]), lambda i, w: (w[0], 0)),
                pl.BlockSpec((rope.shape[0], HALF), lambda i, w: (0, w[0])),
                pl.BlockSpec((1, latent.shape[1]), lambda i, w: (0, 0)),
            ],
            out_specs=pl.BlockSpec((count, 80, HALF), lambda i, w: (0, 0, 0)),
            scratch_shapes=[pltpu.VMEM((channels, HALF), jnp.bfloat16)],
        ),
        cost_estimate=pl.CostEstimate(flops=10**6, bytes_accessed=10**6, transcendentals=HALF),
        compiler_params=pltpu.CompilerParams(vmem_limit_bytes=4 * 2**20),
        name="key_share",
    )(place, latent, rope, gain[None])


def merge_kernel(parts_ref, out_ref, log_ref, turn_ref):
    count, rows = parts_ref.shape[0], out_ref.shape[0]
    heads = out_ref.shape[1] // VD
    turn_ref[...] = jnp.zeros_like(turn_ref)
    for h in range(heads):
        levels = []
        for i in range(count):
            terms = [
                parts_ref[i, rows : rows + EXTRA, :].astype(jnp.float32)[h * 3 + k : h * 3 + k + 1]
                for k in range(3)
            ]
            levels.append(terms[0] + terms[1] + terms[2])
        top = levels[0]
        for level in levels[1:]:
            top = jnp.maximum(top, level)
        shares = [jnp.exp2(level - top) for level in levels]
        total = shares[0]
        for share in shares[1:]:
            total = total + share
        log_ref[h : h + 1, :] = (top + jnp.log2(total)) * LN2
        inverse = 1.0 / total
        for i in range(count):
            turn_ref[h * count + i : h * count + i + 1, :] = shares[i] * inverse
    turned = turn_ref[...].T
    for h in range(heads):
        merged = jnp.zeros((rows, VD), jnp.float32)
        for i in range(count):
            k = h * count + i
            part = parts_ref[i, :rows, h * VD : (h + 1) * VD].astype(jnp.float32)
            merged = merged + part * turned[:, k : k + 1]
        out_ref[:, h * VD : (h + 1) * VD] = merged.astype(out_ref.dtype)


def merge(parts):
    _, rows, channels = parts.shape
    rows -= EXTRA
    vmem = pl.BlockSpec(memory_space=pltpu.VMEM)
    return pl.pallas_call(
        merge_kernel,
        out_shape=[
            jax.ShapeDtypeStruct((rows, channels), jnp.bfloat16),
            jax.ShapeDtypeStruct((channels // VD, rows), jnp.float32),
        ],
        in_specs=[vmem],
        out_specs=[vmem, vmem],
        scratch_shapes=[pltpu.VMEM((128, rows), jnp.float32)],
        cost_estimate=pl.CostEstimate(flops=10**6, bytes_accessed=10**6, transcendentals=10**4),
        compiler_params=pltpu.CompilerParams(vmem_limit_bytes=8 * 2**20),
        name="merge",
    )(parts)


def to_all(value, axis):
    count = lax.axis_size(axis)
    return lax.all_to_all(jnp.broadcast_to(value[None], (count, *value.shape)), axis, 0, 0)


def local(
    q_latent,
    kv_latent,
    key_rope,
    pool_input,
    q_lat_gain,
    kv_lat_gain,
    q_head_gain,
    k_head_gain,
    pool_gain,
    q_up,
    key_up,
    value_up,
    pool_mix,
    out_pool,
    out_attn,
):
    row_count = q_latent.shape[0]
    sp_index = lax.axis_index("sp")
    sp_size = lax.axis_size("sp")
    core = lax.axis_index("tp")
    line = lax.axis_index("fs")
    z, y = lax.div(sp_index, Y), lax.rem(sp_index, Y)
    own_pos = sp_index * row_count + jnp.arange(row_count, dtype=jnp.int32)
    key_groups = [
        [p * Y + n for p in (j, PLANES - 1 - j) for n in range(Y)] for j in range(PLANES // 2)
    ]
    query_groups = [
        [(c + 2 * i) * Y + n for i in range(MEMBERS)] for c in range(2) for n in range(Y)
    ]
    block_cos, block_sin, in_cos, in_sin = turn_tables(row_count, sp_size)
    plane_turns = np.transpose(
        np.concatenate([block_cos, block_sin], axis=1).reshape(-1, Y, ROPE), (0, 2, 1)
    )

    share = key_share(
        jnp.stack([core, line]).astype(jnp.int32), kv_latent, key_rope.T, kv_lat_gain, 2 * Y
    )
    mine = lax.all_to_all(share, "sp", 0, 0, axis_index_groups=key_groups)
    mine = to_all(mine, "fs")
    other = lax.ppermute(mine, "tp", [(0, 1), (1, 0)])

    own_cos = lax.dynamic_slice_in_dim(jnp.asarray(block_cos), sp_index, 1, 0)
    own_sin = lax.dynamic_slice_in_dim(jnp.asarray(block_sin), sp_index, 1, 0)
    queries = make_queries(
        q_latent,
        q_lat_gain,
        q_up,
        q_head_gain,
        k_head_gain,
        own_cos * in_cos - own_sin * in_sin,
        own_sin * in_cos + own_cos * in_sin,
    )

    def turned(d):
        pairs = [(g[i], g[(i + d) % MEMBERS]) for g in query_groups for i in range(MEMBERS)]
        return lax.ppermute(queries, "sp", pairs)

    queries = [queries] + [turned(d) for d in range(1, MEMBERS)]
    within = jnp.asarray(np.stack([in_cos.T, in_sin.T]))
    near = lax.dynamic_slice_in_dim(within, core * HALF, HALF, 2)
    far = lax.dynamic_slice_in_dim(within, HALF - core * HALF, HALF, 2)
    low_plane = jnp.minimum(z, PLANES - 1 - z)
    place = jnp.stack(
        [low_plane, PLANES - 1 - low_plane, lax.rem(z, 2), y, core * HALF, lax.div(z, 2)]
    ).astype(jnp.int32)
    partial_out = attend(
        place,
        mine,
        other,
        queries,
        key_up,
        value_up,
        k_head_gain[None],
        jnp.asarray(plane_turns),
        near,
        far,
    )
    parts = lax.all_to_all(partial_out, "sp", 0, 0, axis_index_groups=query_groups)
    attended, log_weight = merge(parts)

    earlier = lax.ppermute(
        pool_input[row_count - 15 :], "sp", [(i, i + 1) for i in range(sp_size - 1)]
    )
    extended = jnp.concatenate([earlier, pool_input], axis=0).astype(jnp.float32)
    window = jnp.left_shift(jnp.int32(2), line)
    window_sum = jnp.zeros((row_count, pool_input.shape[1]), jnp.float32)
    for lag_rows in range(16):
        window_sum = window_sum + jnp.where(
            lag_rows < window, extended[15 - lag_rows : 15 - lag_rows + row_count], 0.0
        )
    counts = jnp.minimum(own_pos + 1, window).astype(jnp.float32)[:, None]
    pool_diff = (window_sum / counts - extended[15:]).astype(jnp.bfloat16)
    pooled = (
        jnp.dot(pool_diff, pool_mix[0], preferred_element_type=jnp.float32) * pool_gain
    ).astype(jnp.bfloat16)

    lines = lax.axis_size("fs")

    def rows_of(array, part):
        array = array.reshape(lines, 2, -1, array.shape[1])
        array = lax.dynamic_index_in_dim(array, part, 1, False)
        return array.reshape(-1, array.shape[-1])

    def projected(part):
        from_pool = jnp.dot(
            rows_of(pooled, part), out_pool, preferred_element_type=jnp.float32
        )
        return from_pool + jnp.dot(
            rows_of(attended, part), out_attn, preferred_element_type=jnp.float32
        )

    sent = projected(1 - core).astype(jnp.bfloat16)
    received = lax.ppermute(sent, "tp", [(0, 1), (1, 0)])
    kept = projected(core)
    chip = (kept + received.astype(jnp.float32)).astype(jnp.bfloat16)
    chip = lax.all_to_all(chip.reshape(lines, -1, chip.shape[1]), "fs", 0, 0)
    mixed = jnp.sum(chip.astype(jnp.float32), axis=0).astype(jnp.bfloat16)
    return (mixed, log_weight)


def solution(mesh):
    in_specs = (
        P("sp", None),
        P("sp", None),
        P("sp", None),
        P("sp", "fs"),
        P(),
        P(),
        P(),
        P(),
        P(("fs", "tp")),
        P(None, ("fs", "tp")),
        P(None, ("fs", "tp")),
        P(None, ("fs", "tp")),
        P("fs", None, "tp"),
        P(("fs", "tp"), None),
        P(("fs", "tp"), None),
    )
    out_specs = (P(("sp", "fs", "tp"), None), P(("fs", "tp"), "sp"))

    return jax.shard_map(local, mesh=mesh, in_specs=in_specs, out_specs=out_specs, check_vma=False)
```

```python
import math

import jax
import jax.numpy as jnp
import numpy as np
from jax import lax
from jax.experimental import pallas as pl
from jax.experimental.pallas import tpu as pltpu
from jax.sharding import PartitionSpec as P


NOPE = 128
ROPE = 64
VD = 128
EPS = 1e-06
THETA = 10000.0
HUGE = 1e30
LOG2E = math.log2(math.e)
LN2 = math.log(2.0)
HALF = 128
Y = 8
PLANES = 8
MEMBERS = 4
VMEM_LIMIT = 32 * 2**20
SHARE_LIMIT = 58 * 2**20
EXTRA = 16


def turn_tables(block_rows, blocks):
    frequency = 1.0 / THETA ** (np.arange(0, ROPE, 2, dtype=np.float64) / ROPE)
    at_block = (np.arange(blocks) * block_rows)[:, None] * frequency
    within = np.arange(block_rows)[:, None] * frequency
    return [t.astype(np.float32) for a in (at_block, within) for t in (np.cos(a), np.sin(a))]


def row_norm(values, row_gain):
    mean_sq = jnp.mean(values * values, axis=-1, keepdims=True)
    return values * lax.rsqrt(mean_sq + EPS) * row_gain


def make_queries(latent, lat_gain, q_up, norm_gain, key_gain, cosine, sine):
    row_count = latent.shape[0]
    normed = row_norm(latent.astype(jnp.float32), lat_gain).astype(jnp.bfloat16)
    query = jnp.dot(normed, q_up, preferred_element_type=jnp.float32).reshape(
        row_count, -1, NOPE + ROPE
    )
    query = row_norm(query, norm_gain)
    scale = LOG2E * (NOPE + ROPE) ** (-0.5)
    cosine, sine = cosine[:, None, :] * scale, sine[:, None, :] * scale
    a, b = query[..., NOPE : NOPE + ROPE // 2], query[..., NOPE + ROPE // 2 :]
    turned = jnp.concatenate([a * cosine - b * sine, a * sine + b * cosine], axis=-1)
    return jnp.concatenate(
        [
            (query[..., :NOPE] * (key_gain[:NOPE] * scale)).reshape(row_count, -1),
            turned.reshape(row_count, -1),
        ],
        axis=-1,
    ).astype(jnp.bfloat16)


def attend_kernel(place_ref, mine_ref, other_ref, *refs):
    query_refs, refs = refs[:MEMBERS], refs[MEMBERS:]
    up_hbm, gain_ref, table_ref, out_ref, *refs = refs
    q_ref, lat_ref, turn_ref, up_ref, far_keys_ref, sems, *refs = refs
    both_ref, *refs = refs
    heads = up_hbm.shape[2] // NOPE
    max_refs, sum_refs, acc_refs, key_refs, score_refs, top_refs = (
        refs[n * heads : (n + 1) * heads] for n in range(6)
    )
    count = MEMBERS
    rows = query_refs[0].shape[0]
    parity, own_y, offset, member = place_ref[2], place_ref[3], place_ref[4], place_ref[5]
    width = Y * rows
    slices = [pl.ds(n * 128, 128) for n in range(width // 128)]
    chunk = min(4, Y) * HALF

    arrivals = [
        pltpu.make_async_copy(
            query_refs[d], q_ref.at[lax.rem(member + (count - d), count)], sems.at[d]
        )
        for d in range(count)
    ]
    arrivals.append(pltpu.make_async_copy(other_ref, far_keys_ref, sems.at[count]))
    weights = pltpu.make_async_copy(up_hbm, both_ref, sems.at[count + 1])
    weights.start()
    for copy in arrivals:
        copy.start()
    for h in range(heads):
        max_refs[h][...] = jnp.full(max_refs[h].shape, -HUGE, jnp.float32)
        sum_refs[h][...] = jnp.zeros_like(sum_refs[h])
        acc_refs[h][...] = jnp.zeros_like(acc_refs[h])
        key_refs[h][NOPE:, :] = jnp.zeros((256 - NOPE, width), jnp.bfloat16)
    weights.wait()
    up_ref[...] = both_ref[0].T
    gain = jnp.broadcast_to(gain_ref[:, NOPE:], (ROPE, ROPE)).T[:, :1]

    def build_keys(step, plane):
        for u, keys_ref in enumerate((mine_ref, far_keys_ref)):
            in_cos = table_ref[u * ROPE : u * ROPE + ROPE // 2, :]
            in_sin = table_ref[u * ROPE + ROPE // 2 : (u + 1) * ROPE, :]
            block_at = pl.multiple_of((2 + plane) * ROPE, ROPE)
            for n in range(Y):
                at = pl.ds((u * Y + n) * HALF, HALF)
                for x in range(3):
                    lat_ref[x * 80 : (x + 1) * 80, at] = keys_ref[x, step * Y + n]
                last = keys_ref[3, step * Y + n]
                lat_ref[240:256, at] = last[:16]
                raw = last[16:].astype(jnp.float32)
                square = jnp.sum(raw * raw, axis=0, keepdims=True)
                top_refs[0][n : n + 1, u * 128 : (u + 1) * 128] = square
                block_cos = table_ref[pl.ds(block_at, ROPE // 2), n : n + 1]
                block_sin = table_ref[pl.ds(block_at + ROPE // 2, ROPE // 2), n : n + 1]
                cosine = block_cos * in_cos - block_sin * in_sin
                sine = block_sin * in_cos + block_cos * in_sin
                raw = raw * gain
                a, b = raw[: ROPE // 2], raw[ROPE // 2 :]
                turn_ref[: ROPE // 2, at] = a * cosine - b * sine
                turn_ref[ROPE // 2 :, at] = a * sine + b * cosine
            for n in range(Y * HALF // chunk):
                at = pl.ds(u * Y * HALF + n * chunk, chunk)
                raw = jnp.dot(up_ref[...], lat_ref[:, at], preferred_element_type=jnp.float32)
                blocks = range(n * chunk // HALF, (n + 1) * chunk // HALF)
                rope_sq = jnp.concatenate(
                    [top_refs[0][k : k + 1, u * 128 : (u + 1) * 128] for k in blocks], axis=1
                )
                for h in range(heads):
                    part = raw[h * NOPE : (h + 1) * NOPE]
                    square = jnp.sum(part * part, axis=0, keepdims=True) + rope_sq
                    inverse = lax.rsqrt(square * (1.0 / (NOPE + ROPE)) + EPS)
                    key_refs[h][:NOPE, at] = (part * inverse).astype(jnp.bfloat16)
                    key_refs[h][NOPE + h * ROPE : NOPE + (h + 1) * ROPE, at] = (
                        turn_ref[:, at] * inverse
                    ).astype(jnp.bfloat16)

    def score(i, h):
        query = jnp.concatenate(
            [q_ref[i, :, h * NOPE : (h + 1) * NOPE], q_ref[i, :, heads * NOPE :]], axis=1
        )
        scores = jnp.dot(query, key_refs[h][...], preferred_element_type=jnp.float32)
        score_refs[h][...] = scores
        top = scores[:, :128]
        for n in range(1, width // 128):
            top = jnp.maximum(top, scores[:, n * 128 : (n + 1) * 128])
        top_refs[h][:, :128] = top

    def mask(h):
        column = lax.broadcasted_iota(jnp.int32, (rows, width), 1)
        row = lax.broadcasted_iota(jnp.int32, (rows, width), 0)
        half_at = jnp.where(column < Y * HALF, offset, HALF - offset)
        key_at = (column % (Y * HALF)) // HALF * rows + half_at + column % HALF
        seen = key_at <= own_y * rows + row
        scores = jnp.where(seen, score_refs[h][...], -HUGE)
        score_refs[h][...] = scores
        top = scores[:, :128]
        for n in range(1, width // 128):
            top = jnp.maximum(top, scores[:, n * 128 : (n + 1) * 128])
        top_refs[h][:, :128] = top

    def weigh(i, h, following=None):
        before = max_refs[h][i]
        after = jnp.maximum(before, jnp.max(top_refs[h][:, :128], axis=1, keepdims=True))
        factor = jnp.exp2(before - after)
        total = sum_refs[h][i] * factor
        update = acc_refs[h][i] * jnp.concatenate([factor, factor], axis=1)
        top = None
        if following is not None:
            j, other = following
            query = jnp.concatenate(
                [q_ref[j, :, other * NOPE : (other + 1) * NOPE], q_ref[j, :, heads * NOPE :]],
                axis=1,
            )
        for n in range(0, len(slices), 4):
            if following is not None:
                at = slice(n * 128, (n + 4) * 128)
                scores = jnp.dot(query, key_refs[other][:, at], preferred_element_type=jnp.float32)
                score_refs[other][:, at] = scores
                for k in range(4):
                    piece = scores[:, k * 128 : (k + 1) * 128]
                    top = piece if top is None else jnp.maximum(top, piece)
            pieces = []
            for at in slices[n : n + 4]:
                weights = jnp.exp2(score_refs[h][:, at] - after)
                pieces.append(weights.astype(jnp.bfloat16))
                total = total + weights
            update = update + lax.dot_general(
                jnp.concatenate(pieces, axis=1),
                lat_ref[:, n * 128 : (n + 4) * 128],
                (((1,), (1,)), ((), ())),
                preferred_element_type=jnp.float32,
            )
        max_refs[h][i] = after
        sum_refs[h][i] = total
        acc_refs[h][i] = update
        if following is not None:
            top_refs[other][:, :128] = top

    for copy in arrivals:
        copy.wait()

    @pl.loop(0, 2)
    def _(step):
        plane = place_ref[step]
        first = lax.div(plane - parity + 1, 2)

        @pl.when(first < count)
        def _():
            build_keys(step, plane)
            score(first, 0)
            own = plane == parity + 2 * first

            @pl.when(own)
            def _():
                for h in range(1, heads):
                    score(first, h)
                for h in range(heads):
                    mask(h)
                for h in range(heads):
                    weigh(first, h)
                score(jnp.minimum(first + 1, count - 1), 0)

            @pl.loop(jnp.where(own, first + 1, first), count)
            def _(i):
                for h in range(heads):
                    if h + 1 < heads:
                        weigh(i, h, (i, h + 1))
                    else:
                        weigh(i, h, (jnp.minimum(i + 1, count - 1), 0))

    @pl.loop(0, count)
    def _(i):
        out_ref[i, rows:, :] = jnp.zeros((EXTRA, heads * VD), out_ref.dtype)
        for h in range(heads):
            total = jnp.sum(sum_refs[h][i], axis=1, keepdims=True)
            seen = total > 0.0
            total = jnp.where(seen, total, 1.0)
            mean = (acc_refs[h][i] * (1.0 / total)).astype(jnp.bfloat16)
            out_ref[i, :rows, h * VD : (h + 1) * VD] = jnp.dot(
                mean, both_ref[1, :, h * VD : (h + 1) * VD], preferred_element_type=jnp.float32
            ).astype(out_ref.dtype)
            level = jnp.where(seen, max_refs[h][i] + jnp.log2(total), -HUGE).T[:1]
            for term in range(3):
                rounded = level.astype(jnp.bfloat16)
                out_ref[i, pl.ds(rows + h * 3 + term, 1), :] = rounded
                level = level - rounded.astype(jnp.float32)


def attend(place, mine, other, queries, up, gain, table):
    rows, channels = queries[0].shape
    heads = up.shape[2] // NOPE
    vmem = pl.BlockSpec(memory_space=pltpu.VMEM)
    wide = [
        pltpu.VMEM((MEMBERS, rows, 128), jnp.float32),
        pltpu.VMEM((MEMBERS, rows, 128), jnp.float32),
        pltpu.VMEM((MEMBERS, rows, 256), jnp.float32),
        pltpu.VMEM((256, Y * rows), jnp.bfloat16),
        pltpu.VMEM((rows, Y * rows), jnp.float32),
        pltpu.VMEM((rows, 256), jnp.float32),
    ]
    return pl.pallas_call(
        attend_kernel,
        out_shape=jax.ShapeDtypeStruct((MEMBERS, rows + EXTRA, heads * VD), jnp.bfloat16),
        in_specs=[
            pl.BlockSpec(memory_space=pltpu.SMEM),
            vmem,
            *[pl.BlockSpec(memory_space=pl.ANY)] * (1 + MEMBERS + 1),
            *[vmem] * 2,
        ],
        out_specs=vmem,
        scratch_shapes=[
            pltpu.VMEM((MEMBERS, rows, channels), jnp.bfloat16),
            pltpu.VMEM((256, Y * rows), jnp.bfloat16),
            pltpu.VMEM((ROPE, Y * rows), jnp.float32),
            pltpu.VMEM(up.shape[:0:-1], jnp.bfloat16),
            pltpu.VMEM(other.shape, jnp.bfloat16),
            pltpu.SemaphoreType.DMA((MEMBERS + 2,)),
            pltpu.VMEM(up.shape, jnp.bfloat16),
            *[s for s in wide for _ in range(heads)],
        ],
        compiler_params=pltpu.CompilerParams(vmem_limit_bytes=VMEM_LIMIT),
        cost_estimate=pl.CostEstimate(
            flops=5 * 2 * rows * Y * rows * heads * 512,
            bytes_accessed=mine.size * 4,
            transcendentals=5 * rows * Y * rows * heads,
        ),
        name="attend",
    )(place, mine, other, *queries, up, gain, table)


def share_kernel(
    place_ref, latent_ref, rope_ref, gain_ref, out_ref, half_ref, all_ref, scale_ref, sems
):
    channels = latent_ref.shape[1]
    at = pl.ds(pl.multiple_of(place_ref[0] * HALF, HALF), HALF)
    copies = [
        pltpu.make_async_copy(latent_ref.at[at], half_ref, sems.at[0]),
        pltpu.make_async_copy(rope_ref.at[:, at], all_ref.at[pl.ds(channels, ROPE)], sems.at[1]),
        pltpu.make_async_copy(gain_ref, scale_ref, sems.at[2]),
    ]
    for copy in copies:
        copy.start()
    for copy in copies:
        copy.wait()
    normed = row_norm(half_ref[...].astype(jnp.float32), scale_ref[...]).astype(jnp.bfloat16)
    all_ref[:channels] = normed.T
    own = all_ref[pl.ds(pl.multiple_of(place_ref[1] * 80, 16), 80), :]
    for n in range(out_ref.shape[0]):
        out_ref[n] = own


def key_share(place, latent, rope, gain, count):
    channels = latent.shape[1]
    hbm = pl.BlockSpec(memory_space=pl.ANY)
    return pl.pallas_call(
        share_kernel,
        out_shape=jax.ShapeDtypeStruct((count, 80, HALF), jnp.bfloat16),
        in_specs=[pl.BlockSpec(memory_space=pltpu.SMEM), hbm, hbm, hbm],
        out_specs=pl.BlockSpec(memory_space=pltpu.VMEM),
        scratch_shapes=[
            pltpu.VMEM((HALF, channels), jnp.bfloat16),
            pltpu.VMEM((channels + ROPE, HALF), jnp.bfloat16),
            pltpu.VMEM((1, channels), jnp.float32),
            pltpu.SemaphoreType.DMA((3,)),
        ],
        cost_estimate=pl.CostEstimate(flops=10**6, bytes_accessed=10**6, transcendentals=HALF),
        compiler_params=pltpu.CompilerParams(vmem_limit_bytes=SHARE_LIMIT),
        name="key_share",
    )(place, latent, rope, gain[None])


def merge_kernel(parts_ref, out_ref, log_ref, turn_ref):
    count, rows = parts_ref.shape[0], out_ref.shape[0]
    heads = out_ref.shape[1] // VD
    turn_ref[...] = jnp.zeros_like(turn_ref)
    for h in range(heads):
        levels = []
        for i in range(count):
            terms = [
                parts_ref[i, rows : rows + EXTRA, :].astype(jnp.float32)[h * 3 + k : h * 3 + k + 1]
                for k in range(3)
            ]
            levels.append(terms[0] + terms[1] + terms[2])
        top = levels[0]
        for level in levels[1:]:
            top = jnp.maximum(top, level)
        shares = [jnp.exp2(level - top) for level in levels]
        total = shares[0]
        for share in shares[1:]:
            total = total + share
        log_ref[h : h + 1, :] = (top + jnp.log2(total)) * LN2
        inverse = 1.0 / total
        for i in range(count):
            turn_ref[h * count + i : h * count + i + 1, :] = shares[i] * inverse
    turned = turn_ref[...].T
    for h in range(heads):
        merged = jnp.zeros((rows, VD), jnp.float32)
        for i in range(count):
            k = h * count + i
            part = parts_ref[i, :rows, h * VD : (h + 1) * VD].astype(jnp.float32)
            merged = merged + part * turned[:, k : k + 1]
        out_ref[:, h * VD : (h + 1) * VD] = merged.astype(out_ref.dtype)


def merge(parts):
    _, rows, channels = parts.shape
    rows -= EXTRA
    vmem = pl.BlockSpec(memory_space=pltpu.VMEM)
    return pl.pallas_call(
        merge_kernel,
        out_shape=[
            jax.ShapeDtypeStruct((rows, channels), jnp.bfloat16),
            jax.ShapeDtypeStruct((channels // VD, rows), jnp.float32),
        ],
        in_specs=[vmem],
        out_specs=[vmem, vmem],
        scratch_shapes=[pltpu.VMEM((128, rows), jnp.float32)],
        cost_estimate=pl.CostEstimate(flops=10**6, bytes_accessed=10**6, transcendentals=10**4),
        compiler_params=pltpu.CompilerParams(vmem_limit_bytes=8 * 2**20),
        name="merge",
    )(parts)


def to_all(value, axis):
    count = lax.axis_size(axis)
    return lax.all_to_all(jnp.broadcast_to(value[None], (count, *value.shape)), axis, 0, 0)


def local(
    q_latent,
    kv_latent,
    key_rope,
    pool_input,
    q_lat_gain,
    kv_lat_gain,
    q_head_gain,
    k_head_gain,
    pool_gain,
    q_up,
    key_up,
    value_up,
    pool_mix,
    out_pool,
    out_attn,
):
    row_count = q_latent.shape[0]
    sp_index = lax.axis_index("sp")
    sp_size = lax.axis_size("sp")
    core = lax.axis_index("tp")
    line = lax.axis_index("fs")
    z, y = lax.div(sp_index, Y), lax.rem(sp_index, Y)
    own_pos = sp_index * row_count + jnp.arange(row_count, dtype=jnp.int32)
    key_groups = [
        [p * Y + n for p in (j, PLANES - 1 - j) for n in range(Y)] for j in range(PLANES // 2)
    ]
    query_groups = [
        [(c + 2 * i) * Y + n for i in range(MEMBERS)] for c in range(2) for n in range(Y)
    ]
    block_cos, block_sin, in_cos, in_sin = turn_tables(row_count, sp_size)
    plane_turns = np.transpose(
        np.concatenate([block_cos, block_sin], axis=1).reshape(-1, Y, ROPE), (0, 2, 1)
    ).reshape(-1, Y)
    plane_turns = np.pad(plane_turns, ((0, 0), (0, HALF - Y)))
    halves = [np.concatenate([in_cos.T, in_sin.T])[:, c * HALF : (c + 1) * HALF] for c in range(2)]
    tables = np.stack([np.concatenate([halves[c], halves[1 - c], plane_turns]) for c in range(2)])

    seat = jnp.stack([core, line]).astype(jnp.int32)
    share = key_share(seat, kv_latent, key_rope.T, kv_lat_gain, 2 * Y)
    mine = lax.all_to_all(share, "sp", 0, 0, axis_index_groups=key_groups)
    mine = to_all(mine, "fs")
    other = lax.ppermute(mine, "tp", [(0, 1), (1, 0)])

    own_cos = lax.dynamic_slice_in_dim(jnp.asarray(block_cos), sp_index, 1, 0)
    own_sin = lax.dynamic_slice_in_dim(jnp.asarray(block_sin), sp_index, 1, 0)
    queries = make_queries(
        q_latent,
        q_lat_gain,
        q_up,
        q_head_gain,
        k_head_gain,
        own_cos * in_cos - own_sin * in_sin,
        own_sin * in_cos + own_cos * in_sin,
    )

    def turned(d):
        pairs = [(g[i], g[(i + d) % MEMBERS]) for g in query_groups for i in range(MEMBERS)]
        return lax.ppermute(queries, "sp", pairs)

    queries = [queries] + [turned(d) for d in range(1, MEMBERS)]
    low_plane = jnp.minimum(z, PLANES - 1 - z)
    place = jnp.stack(
        [low_plane, PLANES - 1 - low_plane, lax.rem(z, 2), y, core * HALF, lax.div(z, 2)]
    ).astype(jnp.int32)
    partial_out = attend(
        place,
        mine,
        other,
        queries,
        jnp.stack([key_up, value_up]),
        k_head_gain[None],
        lax.dynamic_index_in_dim(jnp.asarray(tables), core, 0, False),
    )
    parts = lax.all_to_all(partial_out, "sp", 0, 0, axis_index_groups=query_groups)
    attended, log_weight = merge(parts)

    earlier = lax.ppermute(
        pool_input[row_count - 15 :], "sp", [(i, i + 1) for i in range(sp_size - 1)]
    )
    extended = jnp.concatenate([earlier, pool_input], axis=0).astype(jnp.float32)
    window = jnp.left_shift(jnp.int32(2), line)
    window_sum = jnp.zeros((row_count, pool_input.shape[1]), jnp.float32)
    for lag_rows in range(16):
        window_sum = window_sum + jnp.where(
            lag_rows < window, extended[15 - lag_rows : 15 - lag_rows + row_count], 0.0
        )
    counts = jnp.minimum(own_pos + 1, window).astype(jnp.float32)[:, None]
    pool_diff = (window_sum / counts - extended[15:]).astype(jnp.bfloat16)
    pooled = (
        jnp.dot(pool_diff, pool_mix[0], preferred_element_type=jnp.float32) * pool_gain
    ).astype(jnp.bfloat16)

    lines = lax.axis_size("fs")

    def rows_of(array, part):
        array = array.reshape(lines, 2, -1, array.shape[1])
        array = lax.dynamic_index_in_dim(array, part, 1, False)
        return array.reshape(-1, array.shape[-1])

    def projected(part):
        from_pool = jnp.dot(
            rows_of(pooled, part), out_pool, preferred_element_type=jnp.float32
        )
        return from_pool + jnp.dot(
            rows_of(attended, part), out_attn, preferred_element_type=jnp.float32
        )

    sent = projected(1 - core).astype(jnp.bfloat16)
    received = lax.ppermute(sent, "tp", [(0, 1), (1, 0)])
    kept = projected(core)
    chip = (kept + received.astype(jnp.float32)).astype(jnp.bfloat16)
    chip = lax.all_to_all(chip.reshape(lines, -1, chip.shape[1]), "fs", 0, 0)
    mixed = jnp.sum(chip.astype(jnp.float32), axis=0).astype(jnp.bfloat16)
    return (mixed, log_weight)


def solution(mesh):
    in_specs = (
        P("sp", None),
        P("sp", None),
        P("sp", None),
        P("sp", "fs"),
        P(),
        P(),
        P(),
        P(),
        P(("fs", "tp")),
        P(None, ("fs", "tp")),
        P(None, ("fs", "tp")),
        P(None, ("fs", "tp")),
        P("fs", None, "tp"),
        P(("fs", "tp"), None),
        P(("fs", "tp"), None),
    )
    out_specs = (P(("sp", "fs", "tp"), None), P(("fs", "tp"), "sp"))

    return jax.shard_map(local, mesh=mesh, in_specs=in_specs, out_specs=out_specs, check_vma=False)
```

```python
import math

import jax
import jax.numpy as jnp
import numpy as np
from jax import lax
from jax.experimental import pallas as pl
from jax.experimental.pallas import tpu as pltpu
from jax.sharding import PartitionSpec as P


NOPE = 128
ROPE = 64
VD = 128
EPS = 1e-06
THETA = 10000.0
HUGE = 1e30
LOG2E = math.log2(math.e)
LN2 = math.log(2.0)
HALF = 128
Y = 8
PLANES = 8
MEMBERS = 4
VMEM_LIMIT = 32 * 2**20
SHARE_LIMIT = 58 * 2**20
EXTRA = 16


def turn_tables(block_rows, blocks):
    frequency = 1.0 / THETA ** (np.arange(0, ROPE, 2, dtype=np.float64) / ROPE)
    at_block = (np.arange(blocks) * block_rows)[:, None] * frequency
    within = np.arange(block_rows)[:, None] * frequency
    return [t.astype(np.float32) for a in (at_block, within) for t in (np.cos(a), np.sin(a))]


def row_norm(values, row_gain):
    mean_sq = jnp.mean(values * values, axis=-1, keepdims=True)
    return values * lax.rsqrt(mean_sq + EPS) * row_gain


def make_queries(latent, lat_gain, q_up, norm_gain, key_gain, cosine, sine):
    row_count = latent.shape[0]
    normed = row_norm(latent.astype(jnp.float32), lat_gain).astype(jnp.bfloat16)
    query = jnp.dot(normed, q_up, preferred_element_type=jnp.float32).reshape(
        row_count, -1, NOPE + ROPE
    )
    query = row_norm(query, norm_gain)
    scale = LOG2E * (NOPE + ROPE) ** (-0.5)
    cosine, sine = cosine[:, None, :] * scale, sine[:, None, :] * scale
    a, b = query[..., NOPE : NOPE + ROPE // 2], query[..., NOPE + ROPE // 2 :]
    turned = jnp.concatenate([a * cosine - b * sine, a * sine + b * cosine], axis=-1)
    return jnp.concatenate(
        [
            (query[..., :NOPE] * (key_gain[:NOPE] * scale)).reshape(row_count, -1),
            turned.reshape(row_count, -1),
        ],
        axis=-1,
    ).astype(jnp.bfloat16)


def attend_kernel(place_ref, mine_ref, other_ref, *refs):
    query_refs, refs = refs[:MEMBERS], refs[MEMBERS:]
    up_hbm, gain_ref, table_ref, out_ref, *refs = refs
    q_ref, lat_ref, turn_ref, up_ref, far_keys_ref, sems, *refs = refs
    both_ref, *refs = refs
    heads = up_hbm.shape[2] // NOPE
    max_refs, sum_refs, acc_refs, key_refs, score_refs, top_refs = (
        refs[n * heads : (n + 1) * heads] for n in range(6)
    )
    count = MEMBERS
    rows = query_refs[0].shape[0]
    parity, own_y, offset, member = place_ref[2], place_ref[3], place_ref[4], place_ref[5]
    width = Y * rows
    slices = [pl.ds(n * 128, 128) for n in range(width // 128)]
    chunk = min(4, Y) * HALF

    arrivals = [
        pltpu.make_async_copy(
            query_refs[d], q_ref.at[lax.rem(member + (count - d), count)], sems.at[d]
        )
        for d in range(count)
    ]
    arrivals.append(pltpu.make_async_copy(other_ref, far_keys_ref, sems.at[count]))
    weights = pltpu.make_async_copy(up_hbm, both_ref, sems.at[count + 1])
    weights.start()
    for copy in arrivals:
        copy.start()
    for h in range(heads):
        max_refs[h][...] = jnp.full(max_refs[h].shape, -HUGE, jnp.float32)
        sum_refs[h][...] = jnp.zeros_like(sum_refs[h])
        acc_refs[h][...] = jnp.zeros_like(acc_refs[h])
        key_refs[h][NOPE:, :] = jnp.zeros((256 - NOPE, width), jnp.bfloat16)
    weights.wait()
    up_ref[...] = both_ref[0].T
    gain = jnp.broadcast_to(gain_ref[:, NOPE:], (ROPE, ROPE)).T[:, :1]

    def build_keys(step, plane):
        for u, keys_ref in enumerate((mine_ref, far_keys_ref)):
            in_cos = table_ref[u * ROPE : u * ROPE + ROPE // 2, :]
            in_sin = table_ref[u * ROPE + ROPE // 2 : (u + 1) * ROPE, :]
            block_at = pl.multiple_of((2 + plane) * ROPE, ROPE)
            for n in range(Y):
                at = pl.ds((u * Y + n) * HALF, HALF)
                for x in range(3):
                    lat_ref[x * 80 : (x + 1) * 80, at] = keys_ref[x, step * Y + n]
                last = keys_ref[3, step * Y + n]
                lat_ref[240:256, at] = last[:16]
                raw = last[16:].astype(jnp.float32)
                square = jnp.sum(raw * raw, axis=0, keepdims=True)
                top_refs[0][n : n + 1, u * 128 : (u + 1) * 128] = square
                block_cos = table_ref[pl.ds(block_at, ROPE // 2), n : n + 1]
                block_sin = table_ref[pl.ds(block_at + ROPE // 2, ROPE // 2), n : n + 1]
                cosine = block_cos * in_cos - block_sin * in_sin
                sine = block_sin * in_cos + block_cos * in_sin
                raw = raw * gain
                a, b = raw[: ROPE // 2], raw[ROPE // 2 :]
                turn_ref[: ROPE // 2, at] = a * cosine - b * sine
                turn_ref[ROPE // 2 :, at] = a * sine + b * cosine
            for n in range(Y * HALF // chunk):
                at = pl.ds(u * Y * HALF + n * chunk, chunk)
                raw = jnp.dot(up_ref[...], lat_ref[:, at], preferred_element_type=jnp.float32)
                blocks = range(n * chunk // HALF, (n + 1) * chunk // HALF)
                rope_sq = jnp.concatenate(
                    [top_refs[0][k : k + 1, u * 128 : (u + 1) * 128] for k in blocks], axis=1
                )
                for h in range(heads):
                    part = raw[h * NOPE : (h + 1) * NOPE]
                    square = jnp.sum(part * part, axis=0, keepdims=True) + rope_sq
                    inverse = lax.rsqrt(square * (1.0 / (NOPE + ROPE)) + EPS)
                    key_refs[h][:NOPE, at] = (part * inverse).astype(jnp.bfloat16)
                    key_refs[h][NOPE + h * ROPE : NOPE + (h + 1) * ROPE, at] = (
                        turn_ref[:, at] * inverse
                    ).astype(jnp.bfloat16)

    def score(i, h):
        query = jnp.concatenate(
            [q_ref[i, :, h * NOPE : (h + 1) * NOPE], q_ref[i, :, heads * NOPE :]], axis=1
        )
        scores = jnp.dot(query, key_refs[h][...], preferred_element_type=jnp.float32)
        score_refs[h][...] = scores
        top = scores[:, :128]
        for n in range(1, width // 128):
            top = jnp.maximum(top, scores[:, n * 128 : (n + 1) * 128])
        top_refs[h][:, :128] = top

    def mask(h):
        column = lax.broadcasted_iota(jnp.int32, (rows, width), 1)
        row = lax.broadcasted_iota(jnp.int32, (rows, width), 0)
        half_at = jnp.where(column < Y * HALF, offset, HALF - offset)
        key_at = (column % (Y * HALF)) // HALF * rows + half_at + column % HALF
        seen = key_at <= own_y * rows + row
        scores = jnp.where(seen, score_refs[h][...], -HUGE)
        score_refs[h][...] = scores
        top = scores[:, :128]
        for n in range(1, width // 128):
            top = jnp.maximum(top, scores[:, n * 128 : (n + 1) * 128])
        top_refs[h][:, :128] = top

    def weigh(i, h, following=None):
        before = max_refs[h][i]
        after = jnp.maximum(before, jnp.max(top_refs[h][:, :128], axis=1, keepdims=True))
        factor = jnp.exp2(before - after)
        total = sum_refs[h][i] * factor
        update = acc_refs[h][i] * jnp.concatenate([factor, factor], axis=1)
        top = None
        if following is not None:
            j, other = following
            query = jnp.concatenate(
                [q_ref[j, :, other * NOPE : (other + 1) * NOPE], q_ref[j, :, heads * NOPE :]],
                axis=1,
            )
        for n in range(0, len(slices), 4):
            if following is not None:
                at = slice(n * 128, (n + 4) * 128)
                scores = jnp.dot(query, key_refs[other][:, at], preferred_element_type=jnp.float32)
                score_refs[other][:, at] = scores
                for k in range(4):
                    piece = scores[:, k * 128 : (k + 1) * 128]
                    top = piece if top is None else jnp.maximum(top, piece)
            pieces = []
            for at in slices[n : n + 4]:
                weights = jnp.exp2(score_refs[h][:, at] - after)
                pieces.append(weights.astype(jnp.bfloat16))
                total = total + weights
            update = update + lax.dot_general(
                jnp.concatenate(pieces, axis=1),
                lat_ref[:, n * 128 : (n + 4) * 128],
                (((1,), (1,)), ((), ())),
                preferred_element_type=jnp.float32,
            )
        max_refs[h][i] = after
        sum_refs[h][i] = total
        acc_refs[h][i] = update
        if following is not None:
            top_refs[other][:, :128] = top

    for copy in arrivals:
        copy.wait()

    @pl.loop(0, 2)
    def _(step):
        plane = place_ref[step]
        first = lax.div(plane - parity + 1, 2)

        @pl.when(first < count)
        def _():
            build_keys(step, plane)
            score(first, 0)
            own = plane == parity + 2 * first

            @pl.when(own)
            def _():
                for h in range(1, heads):
                    score(first, h)
                for h in range(heads):
                    mask(h)
                for h in range(heads):
                    weigh(first, h)
                score(jnp.minimum(first + 1, count - 1), 0)

            @pl.loop(jnp.where(own, first + 1, first), count)
            def _(i):
                for h in range(heads):
                    if h + 1 < heads:
                        weigh(i, h, (i, h + 1))
                    else:
                        weigh(i, h, (jnp.minimum(i + 1, count - 1), 0))

    @pl.loop(0, count)
    def _(i):
        out_ref[i, rows:, :] = jnp.zeros((EXTRA, heads * VD), out_ref.dtype)
        for h in range(heads):
            total = jnp.sum(sum_refs[h][i], axis=1, keepdims=True)
            seen = total > 0.0
            total = jnp.where(seen, total, 1.0)
            mean = (acc_refs[h][i] * (1.0 / total)).astype(jnp.bfloat16)
            out_ref[i, :rows, h * VD : (h + 1) * VD] = jnp.dot(
                mean, both_ref[1, :, h * VD : (h + 1) * VD], preferred_element_type=jnp.float32
            ).astype(out_ref.dtype)
            level = jnp.where(seen, max_refs[h][i] + jnp.log2(total), -HUGE).T[:1]
            for term in range(3):
                rounded = level.astype(jnp.bfloat16)
                out_ref[i, pl.ds(rows + h * 3 + term, 1), :] = rounded
                level = level - rounded.astype(jnp.float32)


def attend(place, mine, other, queries, up, gain, table):
    rows, channels = queries[0].shape
    heads = up.shape[2] // NOPE
    vmem = pl.BlockSpec(memory_space=pltpu.VMEM)
    wide = [
        pltpu.VMEM((MEMBERS, rows, 128), jnp.float32),
        pltpu.VMEM((MEMBERS, rows, 128), jnp.float32),
        pltpu.VMEM((MEMBERS, rows, 256), jnp.float32),
        pltpu.VMEM((256, Y * rows), jnp.bfloat16),
        pltpu.VMEM((rows, Y * rows), jnp.float32),
        pltpu.VMEM((rows, 256), jnp.float32),
    ]
    return pl.pallas_call(
        attend_kernel,
        out_shape=jax.ShapeDtypeStruct((MEMBERS, rows + EXTRA, heads * VD), jnp.bfloat16),
        in_specs=[
            pl.BlockSpec(memory_space=pltpu.SMEM),
            vmem,
            *[pl.BlockSpec(memory_space=pl.ANY)] * (1 + MEMBERS + 1),
            *[vmem] * 2,
        ],
        out_specs=vmem,
        scratch_shapes=[
            pltpu.VMEM((MEMBERS, rows, channels), jnp.bfloat16),
            pltpu.VMEM((256, Y * rows), jnp.bfloat16),
            pltpu.VMEM((ROPE, Y * rows), jnp.float32),
            pltpu.VMEM(up.shape[:0:-1], jnp.bfloat16),
            pltpu.VMEM(other.shape, jnp.bfloat16),
            pltpu.SemaphoreType.DMA((MEMBERS + 2,)),
            pltpu.VMEM(up.shape, jnp.bfloat16),
            *[s for s in wide for _ in range(heads)],
        ],
        compiler_params=pltpu.CompilerParams(vmem_limit_bytes=VMEM_LIMIT),
        cost_estimate=pl.CostEstimate(
            flops=5 * 2 * rows * Y * rows * heads * 512,
            bytes_accessed=mine.size * 4,
            transcendentals=5 * rows * Y * rows * heads,
        ),
        name="attend",
    )(place, mine, other, *queries, up, gain, table)


def share_kernel(
    latent_ref, rope_ref, gain_ref, out_ref, half_ref, all_ref, scale_ref, own_ref, sems
):
    channels = latent_ref.shape[1]
    at = pl.ds(pl.multiple_of(lax.axis_index("tp") * HALF, HALF), HALF)
    copies = [
        pltpu.make_async_copy(latent_ref.at[at], half_ref, sems.at[0]),
        pltpu.make_async_copy(rope_ref.at[:, at], all_ref.at[pl.ds(channels, ROPE)], sems.at[1]),
        pltpu.make_async_copy(gain_ref, scale_ref, sems.at[2]),
    ]
    for copy in copies:
        copy.start()
    for copy in copies:
        copy.wait()
    normed = row_norm(half_ref[...].astype(jnp.float32), scale_ref[...]).astype(jnp.bfloat16)
    all_ref[:channels] = normed.T
    own_ref[...] = all_ref[pl.ds(pl.multiple_of(lax.axis_index("fs") * 80, 16), 80), :]
    copies = [
        pltpu.make_async_copy(own_ref, out_ref.at[n], sems.at[3 + n])
        for n in range(out_ref.shape[0])
    ]
    for copy in copies:
        copy.start()
    for copy in copies:
        copy.wait()


def key_share(latent, rope, gain, count):
    channels = latent.shape[1]
    hbm = pl.BlockSpec(memory_space=pl.ANY)
    return pl.pallas_call(
        share_kernel,
        out_shape=jax.ShapeDtypeStruct((count, 80, HALF), jnp.bfloat16),
        in_specs=[hbm, hbm, hbm],
        out_specs=hbm,
        scratch_shapes=[
            pltpu.VMEM((HALF, channels), jnp.bfloat16),
            pltpu.VMEM((channels + ROPE, HALF), jnp.bfloat16),
            pltpu.VMEM((1, channels), jnp.float32),
            pltpu.VMEM((80, HALF), jnp.bfloat16),
            pltpu.SemaphoreType.DMA((3 + count,)),
        ],
        cost_estimate=pl.CostEstimate(flops=10**6, bytes_accessed=10**6, transcendentals=HALF),
        compiler_params=pltpu.CompilerParams(vmem_limit_bytes=SHARE_LIMIT),
        name="key_share",
    )(latent, rope, gain[None])


def merge_kernel(parts_ref, out_ref, log_ref, turn_ref):
    count, rows = parts_ref.shape[0], out_ref.shape[0]
    heads = out_ref.shape[1] // VD
    turn_ref[...] = jnp.zeros_like(turn_ref)
    for h in range(heads):
        levels = []
        for i in range(count):
            terms = [
                parts_ref[i, rows : rows + EXTRA, :].astype(jnp.float32)[h * 3 + k : h * 3 + k + 1]
                for k in range(3)
            ]
            levels.append(terms[0] + terms[1] + terms[2])
        top = levels[0]
        for level in levels[1:]:
            top = jnp.maximum(top, level)
        shares = [jnp.exp2(level - top) for level in levels]
        total = shares[0]
        for share in shares[1:]:
            total = total + share
        log_ref[h : h + 1, :] = (top + jnp.log2(total)) * LN2
        inverse = 1.0 / total
        for i in range(count):
            turn_ref[h * count + i : h * count + i + 1, :] = shares[i] * inverse
    turned = turn_ref[...].T
    for h in range(heads):
        merged = jnp.zeros((rows, VD), jnp.float32)
        for i in range(count):
            k = h * count + i
            part = parts_ref[i, :rows, h * VD : (h + 1) * VD].astype(jnp.float32)
            merged = merged + part * turned[:, k : k + 1]
        out_ref[:, h * VD : (h + 1) * VD] = merged.astype(out_ref.dtype)


def merge(parts):
    _, rows, channels = parts.shape
    rows -= EXTRA
    vmem = pl.BlockSpec(memory_space=pltpu.VMEM)
    return pl.pallas_call(
        merge_kernel,
        out_shape=[
            jax.ShapeDtypeStruct((rows, channels), jnp.bfloat16),
            jax.ShapeDtypeStruct((channels // VD, rows), jnp.float32),
        ],
        in_specs=[vmem],
        out_specs=[vmem, vmem],
        scratch_shapes=[pltpu.VMEM((128, rows), jnp.float32)],
        cost_estimate=pl.CostEstimate(flops=10**6, bytes_accessed=10**6, transcendentals=10**4),
        compiler_params=pltpu.CompilerParams(vmem_limit_bytes=8 * 2**20),
        name="merge",
    )(parts)


def to_all(value, axis):
    count = lax.axis_size(axis)
    return lax.all_to_all(jnp.broadcast_to(value[None], (count, *value.shape)), axis, 0, 0)


def local(
    q_latent,
    kv_latent,
    key_rope,
    pool_input,
    q_lat_gain,
    kv_lat_gain,
    q_head_gain,
    k_head_gain,
    pool_gain,
    q_up,
    key_up,
    value_up,
    pool_mix,
    out_pool,
    out_attn,
):
    row_count = q_latent.shape[0]
    sp_index = lax.axis_index("sp")
    sp_size = lax.axis_size("sp")
    core = lax.axis_index("tp")
    line = lax.axis_index("fs")
    z, y = lax.div(sp_index, Y), lax.rem(sp_index, Y)
    own_pos = sp_index * row_count + jnp.arange(row_count, dtype=jnp.int32)
    key_groups = [
        [p * Y + n for p in (j, PLANES - 1 - j) for n in range(Y)] for j in range(PLANES // 2)
    ]
    query_groups = [
        [(c + 2 * i) * Y + n for i in range(MEMBERS)] for c in range(2) for n in range(Y)
    ]
    block_cos, block_sin, in_cos, in_sin = turn_tables(row_count, sp_size)
    plane_turns = np.transpose(
        np.concatenate([block_cos, block_sin], axis=1).reshape(-1, Y, ROPE), (0, 2, 1)
    ).reshape(-1, Y)
    plane_turns = np.pad(plane_turns, ((0, 0), (0, HALF - Y)))
    halves = [np.concatenate([in_cos.T, in_sin.T])[:, c * HALF : (c + 1) * HALF] for c in range(2)]
    tables = np.stack([np.concatenate([halves[c], halves[1 - c], plane_turns]) for c in range(2)])

    share = key_share(kv_latent, key_rope.T, kv_lat_gain, 2 * Y)
    mine = lax.all_to_all(share, "sp", 0, 0, axis_index_groups=key_groups)
    mine = to_all(mine, "fs")
    other = lax.ppermute(mine, "tp", [(0, 1), (1, 0)])

    own_cos = lax.dynamic_slice_in_dim(jnp.asarray(block_cos), sp_index, 1, 0)
    own_sin = lax.dynamic_slice_in_dim(jnp.asarray(block_sin), sp_index, 1, 0)
    queries = make_queries(
        q_latent,
        q_lat_gain,
        q_up,
        q_head_gain,
        k_head_gain,
        own_cos * in_cos - own_sin * in_sin,
        own_sin * in_cos + own_cos * in_sin,
    )

    def turned(d):
        pairs = [(g[i], g[(i + d) % MEMBERS]) for g in query_groups for i in range(MEMBERS)]
        return lax.ppermute(queries, "sp", pairs)

    queries = [queries] + [turned(d) for d in range(1, MEMBERS)]
    low_plane = jnp.minimum(z, PLANES - 1 - z)
    place = jnp.stack(
        [low_plane, PLANES - 1 - low_plane, lax.rem(z, 2), y, core * HALF, lax.div(z, 2)]
    ).astype(jnp.int32)
    partial_out = attend(
        place,
        mine,
        other,
        queries,
        jnp.stack([key_up, value_up]),
        k_head_gain[None],
        lax.dynamic_index_in_dim(jnp.asarray(tables), core, 0, False),
    )
    parts = lax.all_to_all(partial_out, "sp", 0, 0, axis_index_groups=query_groups)
    attended, log_weight = merge(parts)

    earlier = lax.ppermute(
        pool_input[row_count - 15 :], "sp", [(i, i + 1) for i in range(sp_size - 1)]
    )
    extended = jnp.concatenate([earlier, pool_input], axis=0).astype(jnp.float32)
    window = jnp.left_shift(jnp.int32(2), line)
    window_sum = jnp.zeros((row_count, pool_input.shape[1]), jnp.float32)
    for lag_rows in range(16):
        window_sum = window_sum + jnp.where(
            lag_rows < window, extended[15 - lag_rows : 15 - lag_rows + row_count], 0.0
        )
    counts = jnp.minimum(own_pos + 1, window).astype(jnp.float32)[:, None]
    pool_diff = (window_sum / counts - extended[15:]).astype(jnp.bfloat16)
    pooled = (
        jnp.dot(pool_diff, pool_mix[0], preferred_element_type=jnp.float32) * pool_gain
    ).astype(jnp.bfloat16)

    lines = lax.axis_size("fs")

    def rows_of(array, part):
        array = array.reshape(lines, 2, -1, array.shape[1])
        array = lax.dynamic_index_in_dim(array, part, 1, False)
        return array.reshape(-1, array.shape[-1])

    def projected(part):
        from_pool = jnp.dot(
            rows_of(pooled, part), out_pool, preferred_element_type=jnp.float32
        )
        return from_pool + jnp.dot(
            rows_of(attended, part), out_attn, preferred_element_type=jnp.float32
        )

    sent = projected(1 - core).astype(jnp.bfloat16)
    received = lax.ppermute(sent, "tp", [(0, 1), (1, 0)])
    kept = projected(core)
    chip = (kept + received.astype(jnp.float32)).astype(jnp.bfloat16)
    chip = lax.all_to_all(chip.reshape(lines, -1, chip.shape[1]), "fs", 0, 0)
    mixed = jnp.sum(chip.astype(jnp.float32), axis=0).astype(jnp.bfloat16)
    return (mixed, log_weight)


def solution(mesh):
    in_specs = (
        P("sp", None),
        P("sp", None),
        P("sp", None),
        P("sp", "fs"),
        P(),
        P(),
        P(),
        P(),
        P(("fs", "tp")),
        P(None, ("fs", "tp")),
        P(None, ("fs", "tp")),
        P(None, ("fs", "tp")),
        P("fs", None, "tp"),
        P(("fs", "tp"), None),
        P(("fs", "tp"), None),
    )
    out_specs = (P(("sp", "fs", "tp"), None), P(("fs", "tp"), "sp"))

    return jax.shard_map(local, mesh=mesh, in_specs=in_specs, out_specs=out_specs, check_vma=False)
```
